32 devices in a mesh: rep: 2 (over x), fs: 8 (over z, y), tp: 2 (over core).
Axes of the slice: x: 2, y: 2, z: 4, core: 2. Of those that a mesh axis runs over, the one named last changes fastest.
Arguments:
- block_input: bfloat16 [8192, 2048], P(('rep', 'fs', 'tp')), may hold values from -6 to 6
- pre_gain: float32 [2048], replicated, may hold values from 0.1 to 1.9
- post_gain: float32 [2048], replicated, may hold values from 0.1 to 1.9
- gate_saved: bfloat16 [8192, 5632], P(('rep', 'fs'), 'tp'), may hold values from -8 to 8
- up_saved: bfloat16 [8192, 5632], P(('rep', 'fs'), 'tp'), may hold values from -6 to 6
- branch_saved: bfloat16 [8192, 2048], P(('rep', 'fs', 'tp')), may hold values from -6 to 6
- out_cotangent: bfloat16 [8192, 2048], P(('rep', 'fs', 'tp')), may hold values from -6 to 6
- gate_weight: bfloat16 [2048, 5632], P('fs', 'tp'), may hold values from -0.125 to 0.125
- up_weight: bfloat16 [2048, 5632], P('fs', 'tp'), may hold values from -0.125 to 0.125
- down_weight: bfloat16 [2048, 5632], P('fs', 'tp'), may hold values from -0.078125 to 0.078125
Outputs:
- input_grad: bfloat16 [8192, 2048], P(('rep', 'fs', 'tp'))
- gate_grad: float32 [2048, 5632], P('fs', 'tp')
- up_grad: float32 [2048, 5632], P('fs', 'tp')
- down_grad: float32 [2048, 5632], P('fs', 'tp')
The draws below stay inside these ranges and needn't reach their ends.
All inputs are finite; a program needn't handle non-finite values.
Results may differ from the reference program's by a relative error of at most 0.018.
Values may be sent and summed in bfloat16 or wider, within the bound.
A program may use at most 128 MiB of HBM per device.

```python
import jax
import jax.numpy as jnp
from jax import lax

D = 2048
FF = 5632
TOKENS = 8192
N_TP = 2


def spiked(array, key, source, target, shards_of, factor):
    owner, partner = [(jnp.arange(array.shape[position]) // (array.shape[position] // shards_of)).reshape([-1 if axis == position else 1 for axis in range(array.ndim)]) for position in (source, target)]
    chosen = jax.random.permutation(key, shards_of)[partner]
    strong = (owner == chosen) | (owner == (partner + shards_of // 2) % shards_of)
    return jnp.where(strong, factor * array, array)


def shard_levels(key, dims, cuts, least, high):
    def one(position, parts):
        draws = jax.random.uniform(jax.random.fold_in(jax.random.fold_in(key, 6), position), (parts,), jnp.float32, least / len(cuts), high / len(cuts))
        return jnp.repeat(jnp.exp(draws), dims[position] // parts).reshape((-1,) + (1,) * (len(dims) - position - 1))

    factor_of = one(*cuts[0])
    for cut in cuts[1:]:
        factor_of = factor_of * one(*cut)
    return factor_of


def centred(key, shape, deviation, reach, pieces=(), dtype=jnp.bfloat16):
    factor_of = shard_levels(key, shape, pieces, -0.22, 0.18) if pieces else 1.0
    values = jax.random.normal(key, shape, jnp.float32) * deviation * factor_of
    return jnp.minimum(jnp.maximum(values, -reach), reach).astype(dtype)


def bell_draw_with(stream_key, dims, deviation, bound, pieces, heavy, dtype=jnp.bfloat16):
    drawn = deviation * jax.random.normal(stream_key, dims, jnp.float32)
    if pieces:
        drawn = drawn * shard_levels(stream_key, dims, pieces, -0.22, 0.18)
    return jnp.clip(spiked(drawn, jax.random.fold_in(stream_key, 3), *heavy), -bound, bound).astype(dtype)


def setup_inputs(seed: int = 0) -> dict:
    streams_of = jax.random.split(jax.random.key(seed), 11)
    return {
        "block_input": centred(streams_of[0], (TOKENS, D), 1.0, 6.0, ((0, 32),)),
        "pre_gain": jnp.clip(1.0 + 0.18 * jax.random.normal(streams_of[1], (D,), jnp.float32), 0.1, 1.9),
        "post_gain": jnp.clip(1.0 + 0.18 * jax.random.normal(streams_of[2], (D,), jnp.float32), 0.1, 1.9),
        "gate_saved": centred(streams_of[3], (TOKENS, FF), 1.5, 8.0, ((0, 16), (1, 2))),
        "up_saved": centred(streams_of[4], (TOKENS, FF), 1.0, 6.0, ((0, 16), (1, 2))),
        "branch_saved": centred(streams_of[5], (TOKENS, D), 1.0, 6.0, ((0, 32),)),
        "out_cotangent": bell_draw_with(streams_of[6], (TOKENS, D), 1.0, 6.0, ((0, 32),), (0, 1, 32, 2.75)),
        "gate_weight": centred(streams_of[7], (D, FF), D ** -0.5, 0.125, ((0, 8), (1, 2))),
        "up_weight": centred(streams_of[8], (D, FF), D ** -0.5, 0.125, ((0, 8), (1, 2))),
        "down_weight": centred(streams_of[9], (D, FF), FF ** -0.5, 0.078125, ((0, 8), (1, 2))),
    }


eps = 1e-06

def contract_rows(left, right):
    return lax.dot_general(left, right, (((0,), (0,)), ((), ())), preferred_element_type=jnp.float32)

def contract_cols(left, right):
    return lax.dot_general(left, right, (((1,), (1,)), ((), ())), preferred_element_type=jnp.float32)

def reference(block_input, pre_gain, post_gain, gate_saved, up_saved, branch_saved, out_cotangent, gate_weight, up_weight, down_weight):
    xfull = block_input.astype(jnp.float32)
    inv_x = lax.rsqrt(lax.optimization_barrier(jnp.mean(xfull * xfull, axis=-1, keepdims=True)) + eps)
    normed = (xfull * inv_x * pre_gain).astype(jnp.bfloat16)
    branch = branch_saved.astype(jnp.float32)
    inv_b = lax.rsqrt(lax.optimization_barrier(jnp.mean(branch * branch, axis=-1, keepdims=True)) + eps)
    upstream = 0.5 * out_cotangent.astype(jnp.float32) * post_gain
    branch_grad = (inv_b * upstream - branch * inv_b ** 3 * lax.optimization_barrier(jnp.mean(upstream * branch, axis=-1, keepdims=True))).astype(jnp.bfloat16)
    gate_f = gate_saved.astype(jnp.float32)
    up_f = up_saved.astype(jnp.float32)
    sigma = jax.nn.sigmoid(gate_f)
    silu_gate = gate_f * sigma
    hidden = (silu_gate * up_f).astype(jnp.bfloat16)
    hidden_grad = jnp.dot(branch_grad, down_weight, preferred_element_type=jnp.float32)
    gate_cot = (hidden_grad * up_f * sigma * (1.0 + gate_f * (1.0 - sigma))).astype(jnp.bfloat16)
    up_cot = (hidden_grad * silu_gate).astype(jnp.bfloat16)
    width = FF // N_TP
    normed_grad = jnp.zeros(xfull.shape, jnp.float32)
    for group in range(N_TP):
        lo = group * width
        partial_sum = contract_cols(gate_cot[:, lo:lo + width], gate_weight[:, lo:lo + width])
        partial_sum = partial_sum + contract_cols(up_cot[:, lo:lo + width], up_weight[:, lo:lo + width])
        normed_grad = normed_grad + lax.optimization_barrier(partial_sum.astype(jnp.bfloat16)).astype(jnp.float32)
    scaled = normed_grad * pre_gain
    input_grad = out_cotangent.astype(jnp.float32) + inv_x * scaled - xfull * inv_x ** 3 * lax.optimization_barrier(jnp.mean(scaled * xfull, axis=-1, keepdims=True))
    gate_grad = contract_rows(normed, gate_cot)
    up_grad = contract_rows(normed, up_cot)
    down_grad = contract_rows(branch_grad, hidden)
    return (input_grad.astype(jnp.bfloat16), gate_grad, up_grad, down_grad)
```

```python
import functools

import jax
import jax.numpy as jnp
from jax import lax
from jax.experimental import pallas as pl
from jax.experimental.pallas import tpu as pltpu
from jax.sharding import PartitionSpec as P

eps = 1e-06
bf16, f32 = jnp.bfloat16, jnp.float32
SEMS, LOCALS = 200, 64


def contract_rows(left, right):
    return lax.dot_general(
        left, right, (((0,), (0,)), ((), ())), preferred_element_type=jnp.float32
    )


def contract_cols(left, right):
    return lax.dot_general(
        left, right, (((1,), (1,)), ((), ())), preferred_element_type=jnp.float32
    )


def shifted(value, reps, step):
    return lax.ppermute(value, "rep", [(i, (i + step) % reps) for i in range(reps)])


def plain_device(
    reps,
    block_input,
    pre_gain,
    post_gain,
    gate_saved,
    up_saved,
    branch_saved,
    out_cotangent,
    gate_weight,
    up_weight,
    down_weight,
):
    me = lax.axis_index("rep")
    width = gate_saved.shape[1] // reps

    def columns(value, owner):
        return lax.dynamic_slice_in_dim(value, owner * width, width, axis=1)

    down_full = lax.all_gather(columns(down_weight, me), "fs", axis=0, tiled=True)

    gates = [columns(gate_saved, me)]
    ups = [columns(up_saved, me)]
    for k in range(1, reps):
        there = lax.rem(me + k, reps)
        gates.append(shifted(columns(gate_saved, there), reps, k))
        ups.append(shifted(columns(up_saved, there), reps, k))

    xfull = block_input.astype(f32)
    inv_x = lax.rsqrt(jnp.mean(xfull * xfull, axis=-1, keepdims=True) + eps)
    normed = (xfull * inv_x * pre_gain).astype(bf16)
    branch = branch_saved.astype(f32)
    inv_b = lax.rsqrt(jnp.mean(branch * branch, axis=-1, keepdims=True) + eps)
    upstream = 0.5 * out_cotangent.astype(f32) * post_gain
    branch_grad = (
        inv_b * upstream - branch * inv_b**3 * jnp.mean(upstream * branch, axis=-1, keepdims=True)
    ).astype(bf16)

    normed_own = [normed] + [shifted(normed, reps, k) for k in range(1, reps)]
    branch_own = [branch_grad] + [shifted(branch_grad, reps, k) for k in range(1, reps)]
    normed_rows = [lax.all_gather(v, "tp", axis=0, tiled=True) for v in normed_own]
    branch_rows = [lax.all_gather(v, "tp", axis=0, tiled=True) for v in branch_own]
    normed_all = jnp.concatenate(normed_rows, axis=0)
    branch_all = jnp.concatenate(branch_rows, axis=0)

    gate_f = jnp.concatenate(gates, axis=0).astype(f32)
    up_f = jnp.concatenate(ups, axis=0).astype(f32)
    sigma = jax.nn.sigmoid(gate_f)
    silu_gate = gate_f * sigma
    hidden = (silu_gate * up_f).astype(bf16)

    def spread(total):
        shard = lax.psum_scatter(total.astype(bf16), "fs", scatter_dimension=0, tiled=True)
        out = jnp.zeros((shard.shape[0], width * reps), f32)
        out = lax.dynamic_update_slice_in_dim(out, shard.astype(f32), me * width, axis=1)
        for k in range(1, reps):
            other = shifted(shard, reps, k).astype(f32)
            out = lax.dynamic_update_slice_in_dim(
                out, other, lax.rem(me - k + reps, reps) * width, axis=1
            )
        return out

    down_grad = spread(contract_rows(branch_all, hidden))

    hidden_grad = jnp.dot(branch_all, down_full, preferred_element_type=f32)
    gate_cot = (hidden_grad * up_f * sigma * (1.0 + gate_f * (1.0 - sigma))).astype(bf16)
    up_cot = (hidden_grad * silu_gate).astype(bf16)
    gate_grad = spread(contract_rows(normed_all, gate_cot))
    up_grad = spread(contract_rows(normed_all, up_cot))

    gate_full = lax.all_gather(columns(gate_weight, me), "fs", axis=0, tiled=True)
    up_full = lax.all_gather(columns(up_weight, me), "fs", axis=0, tiled=True)
    partial = (contract_cols(gate_cot, gate_full) + contract_cols(up_cot, up_full)).astype(bf16)
    rows = partial.shape[0] // reps
    normed_grad = None
    for k in range(reps):
        piece = lax.psum_scatter(
            partial[k * rows : (k + 1) * rows], "tp", scatter_dimension=0, tiled=True
        )
        if k:
            piece = shifted(piece, reps, reps - k)
        piece = piece.astype(f32)
        normed_grad = piece if normed_grad is None else normed_grad + piece

    scaled = normed_grad * pre_gain
    input_grad = (
        out_cotangent.astype(f32)
        + inv_x * scaled
        - xfull * inv_x**3 * jnp.mean(scaled * xfull, axis=-1, keepdims=True)
    )
    return (input_grad.astype(bf16), gate_grad, up_grad, down_grad)


LANE = 128
MESH = pl.DeviceIdType.MESH


class Links:
    def __init__(self, send, recv, local):
        self.send, self.recv, self.local = send, recv, local
        self.names, self.count, self.pending, self.locals = {}, 0, [], 0

    def index(self, name, size=1):
        if name not in self.names:
            self.names[name] = self.count
            self.count += size
        return self.names[name]

    def make(self, name, src, dst, device, size=1, send_at=0, recv_at=0):
        base = self.index(name, size)
        return pltpu.make_async_remote_copy(
            src_ref=src,
            dst_ref=dst,
            send_sem=self.send.at[base + send_at],
            recv_sem=self.recv.at[base + recv_at],
            device_id=device,
            device_id_type=MESH,
        )

    def start(self, name, src, dst, device, when=None, **at):
        copy = self.make(name, src, dst, device, **at)
        guarded(when, copy.start)
        self.pending.append((when, copy))

    def arrive(self, name, dst, device, when=None, **at):
        guarded(when, self.make(name, dst, dst, device, **at).wait_recv)

    def here(self, src, dst, when=None):
        copy = pltpu.make_async_copy(src, dst, self.local.at[self.locals])
        self.locals += 1
        guarded(when, copy.start)
        return lambda: guarded(when, copy.wait)

    def finish(self):
        for when, copy in self.pending:
            guarded(when, copy.wait_send)


def guarded(when, action):
    if when is None:
        action()
    else:
        pl.when(when)(action)


def fused_kernel(
    nz,
    normed,
    branch,
    gate,
    up,
    down_w,
    gate_w,
    up_w,
    down_out,
    gate_out,
    up_out,
    sum_own,
    sum_far,
    rows,
    acts,
    weights,
    parts,
    halves,
    near,
    mate,
    side,
    tile,
    send,
    recv,
    local,
):
    x, f, c = (lax.axis_index(a) for a in ("rep", "fs", "tp"))
    y, z = lax.rem(f, 2), lax.div(f, 2)
    links = Links(send, recv, local)
    to_x = {"rep": 1 - x}
    to_y = {"fs": f + 1 - 2 * y}
    to_d = {"rep": 1 - x, "fs": f + 1 - 2 * y}
    to_c = {"tp": 1 - c}
    to_up, to_dn = {"fs": f + 2}, {"fs": f - 2}
    has_up, has_dn = z < nz - 1, z > 0

    tokens, model = normed.shape
    chip = gate.shape[0]
    feats = down_w.shape[0]
    block = 2 * feats
    half = gate.shape[1] // 2
    full = acts.shape[2]
    main = full - LANE
    cut = full // 2
    wide, slim = y == c, y != c
    sources = (down_w, gate_w, up_w)
    outs = (down_out, gate_out, up_out)

    def lanes(start, size):
        return pl.ds(pl.multiple_of(start, LANE), size)

    barrier = pltpu.get_barrier_semaphore()
    for device in (to_x, to_y, to_d, to_c):
        pl.semaphore_signal(barrier, inc=1, device_id=device, device_id_type=MESH)

    @pl.when(has_up)
    def _():
        pl.semaphore_signal(barrier, inc=1, device_id=to_up, device_id_type=MESH)

    @pl.when(has_dn)
    def _():
        pl.semaphore_signal(barrier, inc=1, device_id=to_dn, device_id_type=MESH)

    def own_cols(xx, yy, lo, hi):
        return lanes(xx * half + yy * (main + LANE) + lo, hi - lo)

    def extra_cols(xx):
        return lanes(xx * half + main, LANE)

    my_feats = pl.ds(f * feats, feats)
    own_weight = []
    for w in range(3):
        own_weight.append(
            (
                links.here(
                    sources[w].at[:, own_cols(x, y, 0, main)],
                    weights.at[w, my_feats, pl.ds(0, main)],
                ),
                links.here(
                    sources[w].at[:, extra_cols(x)],
                    weights.at[w, my_feats, pl.ds(main, LANE)],
                    wide,
                ),
            )
        )
    own_acts = []
    for g, saved in ((1, gate), (2, up)):
        own_acts.append(
            links.here(saved.at[:, own_cols(x, y, 0, main)], acts.at[g, pl.ds(0, chip), pl.ds(0, main)])
        )
        own_acts.append(
            links.here(
                saved.at[:, extra_cols(x)], acts.at[g, pl.ds(0, chip), pl.ds(main, LANE)], wide
            )
        )

    def slot_rows(slot, core):
        return pl.ds((slot * 2 + core) * tokens, tokens)

    own_rows = [
        links.here(branch, rows.at[0, slot_rows(0, c), :]),
        links.here(normed, rows.at[1, slot_rows(0, c), :]),
    ]

    pl.semaphore_wait(barrier, 4 + has_up.astype(jnp.int32) + has_dn.astype(jnp.int32))

    tables = (branch, normed)
    part = model // 2

    def row_cols(h):
        return pl.ds(h * part, part)

    def row_send(a, kind):
        h = 0 if kind in ("y1", "x2", "x3") else 1
        device = to_y if kind[0] == "y" else to_x
        if kind in ("x3", "y3"):
            source = rows.at[a, slot_rows(1 if kind == "x3" else 2, c), row_cols(h)]
            target = 3
        else:
            source = tables[a].at[:, row_cols(h)]
            target = 1 if kind[0] == "y" else 2
        links.start(f"r{a}{kind}", source, rows.at[a, slot_rows(target, c), row_cols(h)], device)

    def row_wait(a, kind):
        h = 0 if kind in ("y1", "x2", "x3") else 1
        device = to_y if kind[0] == "y" else to_x
        target = 3 if kind in ("x3", "y3") else (1 if kind[0] == "y" else 2)
        links.arrive(f"r{a}{kind}", rows.at[a, slot_rows(target, c), row_cols(h)], device)

    def mate_send(a, slot):
        where = rows.at[a, slot_rows(slot, c), :]
        source = tables[a] if slot == 0 else where
        links.start(f"m{a}{slot}", source, where, to_c)

    def mate_wait(a, slot):
        links.arrive(f"m{a}{slot}", rows.at[a, slot_rows(slot, 1 - c), :], to_c)

    def y_weight(w):
        there = weights.at[w, my_feats, :]
        links.start(
            f"w{w}y",
            sources[w].at[:, own_cols(x, 1 - y, 0, main)],
            there.at[:, pl.ds(0, main)],
            to_y,
        )
        links.start(
            f"w{w}e", sources[w].at[:, extra_cols(x)], there.at[:, pl.ds(main, LANE)], to_y, slim
        )

    def y_weight_wait(w):
        there = weights.at[w, pl.ds((f + 1 - 2 * y) * feats, feats), :]
        links.arrive(f"w{w}y", there.at[:, pl.ds(0, main)], to_y)
        links.arrive(f"w{w}e", there.at[:, pl.ds(main, LANE)], to_y, wide)

    def weight_piece(w, origin, o, width):
        yy = y if o == 0 else 1 - y
        return weights.at[w, pl.ds((origin * 2 + yy) * feats, feats), pl.ds(0, width)]

    def z_send(w, o, hop):
        for width, size in ((full, wide), (main, slim)):
            ahead = weight_piece(w, jnp.maximum(z - hop, 0), o, width)
            when = size & has_up & (z >= hop)
            links.start(f"z{w}{o}u{hop}", ahead, ahead, to_up, when)
            behind = weight_piece(w, jnp.minimum(z + hop, nz - 1), o, width)
            when = size & has_dn & (z + hop < nz)
            links.start(f"z{w}{o}d{hop}", behind, behind, to_dn, when)

    def z_wait(w, o, hop):
        for width, size in ((full, wide), (main, slim)):
            ahead = weight_piece(w, jnp.maximum(z - hop, 0), o, width)
            links.arrive(f"z{w}{o}u{hop - 1}", ahead, to_up, size & (z >= hop))
            behind = weight_piece(w, jnp.minimum(z + hop, nz - 1), o, width)
            links.arrive(f"z{w}{o}d{hop - 1}", behind, to_dn, size & (z + hop < nz))

    def z_step(w, o, hop):
        z_wait(w, o, hop)
        if hop < nz - 1:
            z_send(w, o, hop)

    peers = ((2, to_x, 1 - x, y), (1, to_y, x, 1 - y), (3, to_d, 1 - x, 1 - y))

    def act_send(q):
        for slot, device, xx, yy in peers:
            for g, saved in ((1, gate), (2, up)):
                there = acts.at[g, pl.ds(slot * chip, chip), :]
                lo, hi = (0, cut) if q == 0 else (cut, main)
                links.start(
                    f"a{q}{g}{slot}",
                    saved.at[:, own_cols(xx, yy, lo, hi)],
                    there.at[:, pl.ds(lo, hi - lo)],
                    device,
                )
                if q == 1:
                    links.start(
                        f"e{g}{slot}",
                        saved.at[:, extra_cols(xx)],
                        there.at[:, pl.ds(main, LANE)],
                        device,
                        yy == c,
                    )

    def act_wait(q):
        for slot, device, _, _ in peers:
            for g in (1, 2):
                there = acts.at[g, pl.ds(slot * chip, chip), :]
                lo, hi = (0, cut) if q == 0 else (cut, main)
                links.arrive(f"a{q}{g}{slot}", there.at[:, pl.ds(lo, hi - lo)], device)
                if q == 1:
                    links.arrive(f"e{g}{slot}", there.at[:, pl.ds(main, LANE)], device, wide)

    total = acts.shape[1]

    def make_hidden(q):
        cols = pl.ds(q * cut, cut)

        @pl.loop(0, total // 64)
        def _(i):
            at = pl.ds(i * 64, 64)
            g = acts[1, at, cols].astype(f32)
            u = acts[2, at, cols].astype(f32)
            acts[0, at, cols] = (g * jax.nn.sigmoid(g) * u).astype(bf16)

    def make_cots(q):
        cols = pl.ds(q * cut, cut)

        @pl.loop(0, total // 256)
        def _(i):
            at = pl.ds(i * 256, 256)
            tile[pl.ds(0, 256), :] = jnp.dot(
                rows[0, at, :], weights[0, :, cols], preferred_element_type=f32
            )

            @pl.loop(0, 4)
            def _(j):
                sub = pl.ds(i * 256 + j * 64, 64)
                grad = tile[pl.ds(j * 64, 64), :]
                g = acts[1, sub, cols].astype(f32)
                u = acts[2, sub, cols].astype(f32)
                s = jax.nn.sigmoid(g)
                acts[1, sub, cols] = (grad * u * s * (1.0 + g * (1.0 - s))).astype(bf16)
                acts[2, sub, cols] = (grad * (g * s)).astype(bf16)

    def order(s):
        def low(zz):
            return jnp.where(
                s < nz - 1 - zz, nz - 1 - s, jnp.where(s == nz - 1, zz, s - (nz - 1 - zz))
            )

        return jnp.where(2 * z < nz, low(z), nz - 1 - low(nz - 1 - z))

    def grad_step(q, g, s):
        d = order(s)
        cols = lanes(q * cut, cut)

        @pl.loop(0, block // 256)
        def _(m):
            tile[pl.ds(m * 256, 256), :] = contract_rows(
                rows[jnp.minimum(g, 1), :, pl.ds(pl.multiple_of(d * block + m * 256, 256), 256)],
                acts[g, :, cols],
            )

        sizes = ((cut, (q == 0) | wide), (cut - LANE, (q == 1) & slim))
        spot = (q * 3 + g) * (nz + 1)
        count = 6 * (nz + 1)

        def take(slot, when):
            for width, size in sizes:
                links.arrive(
                    "p",
                    parts.at[g, slot, :, lanes(q * cut, width)],
                    to_up,
                    when & size,
                    size=count,
                    recv_at=spot + slot,
                )

        far = d != z
        fed = jnp.where(d > z, has_dn, jnp.where(d < z, has_up, has_dn))
        take(d, fed)

        @pl.loop(0, block // 64)
        def _(i):
            at = pl.ds(i * 64, 64)

            @pl.when(fed)
            def _():
                tile[at, :] += parts[g, d, at, cols].astype(f32)

        take(nz, (d == z) & has_up)

        @pl.when((d == z) & has_up)
        def _():
            @pl.loop(0, block // 64)
            def _(i):
                at = pl.ds(i * 64, 64)
                tile[at, :] += parts[g, nz, at, cols].astype(f32)

        @pl.loop(0, block // 64)
        def _(i):
            at = pl.ds(i * 64, 64)
            parts[g, d, at, cols] = tile[at, :].astype(bf16)

        target = jnp.where(d == z - 1, nz, d)
        device = {"fs": jnp.where(d > z, f + 2, f - 2)}
        for width, size in sizes:
            copy = links.make(
                "p",
                parts.at[g, d, :, lanes(q * cut, width)],
                parts.at[g, target, :, lanes(q * cut, width)],
                device,
                size=count,
                send_at=spot + d,
                recv_at=spot + target,
            )
            guarded(far & size, copy.start)

    def grad_sent():
        @pl.loop(0, 6)
        def _(i):
            q, g = lax.div(i, 3), lax.rem(i, 3)
            spot = i * (nz + 1)

            @pl.loop(0, nz)
            def _(d):
                for width, size in (
                    (cut, (q == 0) | wide),
                    (cut - LANE, (q == 1) & slim),
                ):
                    copy = links.make(
                        "p",
                        parts.at[g, d, :, lanes(q * cut, width)],
                        parts.at[g, d, :, lanes(q * cut, width)],
                        to_up,
                        send_at=spot + d,
                        recv_at=spot + d,
                    )
                    guarded((d != z) & size, copy.wait_send)

    out_waits = []

    def mine(g, yy, lo, hi):
        return lanes(yy * (main + LANE) + lo, hi - lo)

    def spread(q, g):
        lo, hi = (0, cut) if q == 0 else (cut, main)

        @pl.loop(0, feats // 64)
        def _(i):
            at = pl.ds(i * 64, 64)
            src = pl.ds(y * feats + i * 64, 64)
            halves[g, at, mine(g, y, lo, hi)] = parts[g, z, src, pl.ds(lo, hi - lo)]

        if q == 1:

            @pl.when(wide)
            def _():
                @pl.loop(0, feats // 64)
                def _(i):
                    at = pl.ds(i * 64, 64)
                    src = pl.ds(y * feats + i * 64, 64)
                    halves[g, at, pl.ds(main, LANE)] = parts[g, z, src, pl.ds(main, LANE)]

        send_rows = parts.at[g, z, pl.ds((1 - y) * feats, feats), :]
        links.start(
            f"h{q}{g}y", send_rows.at[:, pl.ds(lo, hi - lo)], halves.at[g, :, mine(g, y, lo, hi)], to_y
        )
        if q == 1:
            links.start(
                f"h{g}e",
                send_rows.at[:, pl.ds(main, LANE)],
                halves.at[g, :, pl.ds(main, LANE)],
                to_y,
                wide,
            )
        leave(q, g, "o", mine(g, y, lo, hi), y * (main + LANE) + lo, hi - lo)

    def leave(q, g, tag, cols, start, size):
        there = outs[g].at[:, lanes(x * half + start, size)]
        links.start(f"h{q}{g}{tag}", halves.at[g, :, cols], there, to_x)
        out_waits.append(links.here(halves.at[g, :, cols], there))
        back = outs[g].at[:, lanes((1 - x) * half + start, size)]
        out_waits.append(lambda: links.arrive(f"h{q}{g}{tag}", back, to_x))

    def spread_on(q, g):
        lo, hi = (0, cut) if q == 0 else (cut, main)
        links.arrive(f"h{q}{g}y", halves.at[g, :, mine(g, 1 - y, lo, hi)], to_y)
        leave(q, g, "n", mine(g, 1 - y, lo, hi), (1 - y) * (main + LANE) + lo, hi - lo)
        if q == 1:
            links.arrive(f"h{g}e", halves.at[g, :, pl.ds(main, LANE)], to_y, slim)
            leave(q, g, "e", pl.ds(main, LANE), main, LANE)

    def row_grad(core, target, add):
        @pl.loop(0, 16)
        def _(i):
            k, n = lax.div(i, 4), lax.rem(i, 4)
            slot = lax.rem(k * 2 + 1, 4) - lax.div(k, 2)
            at = pl.ds((slot * 2 + core) * tokens, tokens)
            wide_cols = pl.ds(pl.multiple_of(n * (model // 4), 512), model // 4)
            feat_rows = pl.ds(n * (model // 4), model // 4)
            value = contract_cols(acts[1, at, :], weights[1, feat_rows, :])
            value = value + contract_cols(acts[2, at, :], weights[2, feat_rows, :])
            if add:
                value = value + mate[slot, :, wide_cols].astype(f32)
            target[slot, :, wide_cols] = value.astype(bf16)

    def add_into(target, source):
        @pl.loop(0, tokens // 32)
        def _(i):
            at = pl.ds(i * 32, 32)
            target[at, :] = (target[at, :].astype(f32) + source[at, :].astype(f32)).astype(bf16)

    mate_send(0, 0)
    mate_send(1, 0)
    y_weight(0)
    for kind in ("y1", "x1", "x2", "y2"):
        row_send(0, kind)
    for wait in own_weight[0]:
        wait()
    z_send(0, 0, 0)
    y_weight_wait(0)
    z_send(0, 1, 0)
    row_wait(0, "x1")
    row_send(0, "y3")
    row_wait(0, "y1")
    row_send(0, "x3")
    act_send(0)
    for kind in ("y1", "x1", "x2", "y2"):
        row_send(1, kind)

    @pl.when(slim)
    def _():
        @pl.loop(0, total // 64)
        def _(i):
            at = pl.ds(i * 64, 64)
            for g in (1, 2):
                acts[g, at, pl.ds(main, LANE)] = jnp.zeros((64, LANE), bf16)

        @pl.loop(0, model // 64)
        def _(i):
            at = pl.ds(i * 64, 64)
            for w in range(3):
                weights[w, at, pl.ds(main, LANE)] = jnp.zeros((64, LANE), bf16)

    z_step(0, 0, 1)
    z_step(0, 1, 1)
    row_wait(0, "y2")
    mate_send(0, 1)
    row_wait(0, "x2")
    mate_send(0, 2)
    z_step(0, 0, 2)
    z_step(0, 1, 2)
    for w in (1, 2):
        for wait in own_weight[w]:
            wait()
        z_send(w, 0, 0)
    row_wait(0, "x3")
    row_wait(0, "y3")
    mate_send(0, 3)
    z_step(0, 0, 3)
    z_step(0, 1, 3)
    for w in (1, 2):
        z_step(w, 0, 1)
    for wait in own_acts + own_rows:
        wait()
    act_wait(0)
    make_hidden(0)
    for slot in range(4):
        mate_wait(0, slot)
    row_wait(1, "x1")
    row_send(1, "y3")
    row_wait(1, "y1")
    row_send(1, "x3")
    y_weight(1)
    y_weight(2)
    act_send(1)

    @pl.loop(0, 2)
    def _(i):
        grad_step(0, 0, i)

    for w in (1, 2):
        z_step(w, 0, 2)
    make_cots(0)

    @pl.loop(2, 4)
    def _(i):
        grad_step(0, 0, i)

    spread(0, 0)
    row_wait(1, "y2")
    mate_send(1, 1)
    row_wait(1, "x2")
    mate_send(1, 2)
    row_wait(1, "x3")
    row_wait(1, "y3")
    mate_send(1, 3)
    for w in (1, 2):
        z_step(w, 0, 3)
    for slot in range(4):
        mate_wait(1, slot)

    @pl.loop(0, 4)
    def _(i):
        grad_step(0, 1 + lax.rem(i, 2), lax.div(i, 2))

    spread_on(0, 0)
    for w in (1, 2):
        y_weight_wait(w)
        z_send(w, 1, 0)
    act_wait(1)
    make_hidden(1)

    @pl.loop(0, 1)
    def _(i):
        grad_step(1, 0, i)

    make_cots(1)

    @pl.loop(4, 8)
    def _(i):
        grad_step(0, 1 + lax.rem(i, 2), lax.div(i, 2))

    spread(0, 1)
    spread(0, 2)
    for w in (1, 2):
        z_step(w, 1, 1)

    @pl.loop(1, 6)
    def _(i):
        grad_step(1, lax.rem(i, 3), lax.div(i, 3))

    spread_on(0, 1)
    spread_on(0, 2)
    for w in (1, 2):
        z_step(w, 1, 2)
    for w in (1, 2):
        z_step(w, 1, 3)
    row_grad(1 - c, near, False)
    for slot in range(4):
        links.start(f"s{slot}", near.at[slot], mate.at[slot], to_c)

    @pl.loop(6, 9)
    def _(i):
        grad_step(1, lax.rem(i, 3), lax.div(i, 3))

    for slot in range(4):
        links.arrive(f"s{slot}", mate.at[slot], to_c)
    row_grad(c, mate, True)
    for i in range(2):
        links.start(f"t{i}", mate.at[2 * i + 1], side.at[i], to_y)

    @pl.loop(9, 12)
    def _(i):
        grad_step(1, lax.rem(i, 3), lax.div(i, 3))

    for g in range(3):
        spread(1, g)
    links.arrive("t1", side.at[1], to_y)
    add_into(mate.at[2], side.at[1])
    links.start("t2", mate.at[2], sum_far, to_x)
    links.arrive("t0", side.at[0], to_y)
    add_into(mate.at[0], side.at[0])
    out_waits.append(links.here(mate.at[0], sum_own))
    for g in range(3):
        spread_on(1, g)
    links.arrive("t2", sum_far, to_x)
    for wait in out_waits:
        wait()
    grad_sent()
    links.finish()


def fused_device(nz, block_input, pre_gain, post_gain, gate_saved, up_saved, branch_saved,
                 out_cotangent, gate_weight, up_weight, down_weight):
    xfull = block_input.astype(f32)
    inv_x = lax.rsqrt(jnp.mean(xfull * xfull, axis=-1, keepdims=True) + eps)
    normed = (xfull * inv_x * pre_gain).astype(bf16)
    branch = branch_saved.astype(f32)
    inv_b = lax.rsqrt(jnp.mean(branch * branch, axis=-1, keepdims=True) + eps)
    upstream = 0.5 * out_cotangent.astype(f32) * post_gain
    branch_grad = (
        inv_b * upstream - branch * inv_b**3 * jnp.mean(upstream * branch, axis=-1, keepdims=True)
    ).astype(bf16)

    tokens, model = block_input.shape
    chip, width = gate_saved.shape
    feats = down_weight.shape[0]
    half = width // 2
    full = (half // LANE + 1) // 2 * LANE
    grad = jax.ShapeDtypeStruct((feats, width), bf16)
    total = jax.ShapeDtypeStruct((tokens, model), bf16)
    down_grad, gate_grad, up_grad, sum_own, sum_far = pl.pallas_call(
        functools.partial(fused_kernel, nz),
        out_shape=(grad, grad, grad, total, total),
        in_specs=[pl.BlockSpec(memory_space=pl.ANY)] * 7,
        out_specs=[pl.BlockSpec(memory_space=pl.ANY)] * 5,
        scratch_shapes=[
            pltpu.VMEM((2, 4 * chip, model), bf16),
            pltpu.VMEM((3, 4 * chip, full), bf16),
            pltpu.VMEM((3, model, full), bf16),
            pltpu.VMEM((3, nz + 1, 2 * feats, full), bf16),
            pltpu.VMEM((3, feats, half), bf16),
            pltpu.VMEM((4, tokens, model), bf16),
            pltpu.VMEM((4, tokens, model), bf16),
            pltpu.VMEM((2, tokens, model), bf16),
            pltpu.VMEM((2 * feats, full // 2), f32),
            pltpu.SemaphoreType.DMA((SEMS,)),
            pltpu.SemaphoreType.DMA((SEMS,)),
            pltpu.SemaphoreType.DMA((LOCALS,)),
        ],
        compiler_params=pltpu.CompilerParams(
            collective_id=0, has_side_effects=True, vmem_limit_bytes=66_900_000
        ),
    )(normed, branch_grad, gate_saved, up_saved, down_weight, gate_weight, up_weight)

    normed_grad = sum_own.astype(f32) + sum_far.astype(f32)
    scaled = normed_grad * pre_gain
    input_grad = (
        out_cotangent.astype(f32)
        + inv_x * scaled
        - xfull * inv_x**3 * jnp.mean(scaled * xfull, axis=-1, keepdims=True)
    )
    return (
        input_grad.astype(bf16),
        gate_grad.astype(f32),
        up_grad.astype(f32),
        down_grad.astype(f32),
    )


def solution(mesh):
    shape = mesh.shape

    def run(*args):
        width = args[3].shape[1] // shape["tp"]
        tiles, odd = divmod(width // 2, LANE)
        fits = shape["rep"] == 2 and shape["tp"] == 2 and shape["fs"] % 2 == 0
        fits = fits and width % 2 == 0 and odd == 0 and tiles % 4 == 3
        if fits:
            per_device = functools.partial(fused_device, shape["fs"] // 2)
        else:
            per_device = functools.partial(plain_device, shape["rep"])
        return jax.shard_map(
            per_device,
            mesh=mesh,
            in_specs=(
                P(("rep", "fs", "tp"), None),
                P(),
                P(),
                P(("rep", "fs"), "tp"),
                P(("rep", "fs"), "tp"),
                P(("rep", "fs", "tp"), None),
                P(("rep", "fs", "tp"), None),
                P("fs", "tp"),
                P("fs", "tp"),
                P("fs", "tp"),
            ),
            out_specs=(P(("rep", "fs", "tp"), None), P("fs", "tp"), P("fs", "tp"), P("fs", "tp")),
            check_vma=False,
        )(*args)

    return run
```

```python
import functools

import jax
import jax.numpy as jnp
from jax import lax
from jax.experimental import pallas as pl
from jax.experimental.pallas import tpu as pltpu
from jax.sharding import PartitionSpec as P

eps = 1e-06
bf16, f32 = jnp.bfloat16, jnp.float32
SEMS, LOCALS = 240, 64
CHUNKS = 3


def contract_rows(left, right):
    return lax.dot_general(
        left, right, (((0,), (0,)), ((), ())), preferred_element_type=jnp.float32
    )


def contract_cols(left, right):
    return lax.dot_general(
        left, right, (((1,), (1,)), ((), ())), preferred_element_type=jnp.float32
    )


def shifted(value, reps, step):
    return lax.ppermute(value, "rep", [(i, (i + step) % reps) for i in range(reps)])


def plain_device(
    reps,
    block_input,
    pre_gain,
    post_gain,
    gate_saved,
    up_saved,
    branch_saved,
    out_cotangent,
    gate_weight,
    up_weight,
    down_weight,
):
    me = lax.axis_index("rep")
    width = gate_saved.shape[1] // reps

    def columns(value, owner):
        return lax.dynamic_slice_in_dim(value, owner * width, width, axis=1)

    down_full = lax.all_gather(columns(down_weight, me), "fs", axis=0, tiled=True)

    gates = [columns(gate_saved, me)]
    ups = [columns(up_saved, me)]
    for k in range(1, reps):
        there = lax.rem(me + k, reps)
        gates.append(shifted(columns(gate_saved, there), reps, k))
        ups.append(shifted(columns(up_saved, there), reps, k))

    xfull = block_input.astype(f32)
    inv_x = lax.rsqrt(jnp.mean(xfull * xfull, axis=-1, keepdims=True) + eps)
    normed = (xfull * inv_x * pre_gain).astype(bf16)
    branch = branch_saved.astype(f32)
    inv_b = lax.rsqrt(jnp.mean(branch * branch, axis=-1, keepdims=True) + eps)
    upstream = 0.5 * out_cotangent.astype(f32) * post_gain
    branch_grad = (
        inv_b * upstream - branch * inv_b**3 * jnp.mean(upstream * branch, axis=-1, keepdims=True)
    ).astype(bf16)

    normed_own = [normed] + [shifted(normed, reps, k) for k in range(1, reps)]
    branch_own = [branch_grad] + [shifted(branch_grad, reps, k) for k in range(1, reps)]
    normed_rows = [lax.all_gather(v, "tp", axis=0, tiled=True) for v in normed_own]
    branch_rows = [lax.all_gather(v, "tp", axis=0, tiled=True) for v in branch_own]
    normed_all = jnp.concatenate(normed_rows, axis=0)
    branch_all = jnp.concatenate(branch_rows, axis=0)

    gate_f = jnp.concatenate(gates, axis=0).astype(f32)
    up_f = jnp.concatenate(ups, axis=0).astype(f32)
    sigma = jax.nn.sigmoid(gate_f)
    silu_gate = gate_f * sigma
    hidden = (silu_gate * up_f).astype(bf16)

    def spread(total):
        shard = lax.psum_scatter(total.astype(bf16), "fs", scatter_dimension=0, tiled=True)
        out = jnp.zeros((shard.shape[0], width * reps), f32)
        out = lax.dynamic_update_slice_in_dim(out, shard.astype(f32), me * width, axis=1)
        for k in range(1, reps):
            other = shifted(shard, reps, k).astype(f32)
            out = lax.dynamic_update_slice_in_dim(
                out, other, lax.rem(me - k + reps, reps) * width, axis=1
            )
        return out

    down_grad = spread(contract_rows(branch_all, hidden))

    hidden_grad = jnp.dot(branch_all, down_full, preferred_element_type=f32)
    gate_cot = (hidden_grad * up_f * sigma * (1.0 + gate_f * (1.0 - sigma))).astype(bf16)
    up_cot = (hidden_grad * silu_gate).astype(bf16)
    gate_grad = spread(contract_rows(normed_all, gate_cot))
    up_grad = spread(contract_rows(normed_all, up_cot))

    gate_full = lax.all_gather(columns(gate_weight, me), "fs", axis=0, tiled=True)
    up_full = lax.all_gather(columns(up_weight, me), "fs", axis=0, tiled=True)
    partial = (contract_cols(gate_cot, gate_full) + contract_cols(up_cot, up_full)).astype(bf16)
    rows = partial.shape[0] // reps
    normed_grad = None
    for k in range(reps):
        piece = lax.psum_scatter(
            partial[k * rows : (k + 1) * rows], "tp", scatter_dimension=0, tiled=True
        )
        if k:
            piece = shifted(piece, reps, reps - k)
        piece = piece.astype(f32)
        normed_grad = piece if normed_grad is None else normed_grad + piece

    scaled = normed_grad * pre_gain
    input_grad = (
        out_cotangent.astype(f32)
        + inv_x * scaled
        - xfull * inv_x**3 * jnp.mean(scaled * xfull, axis=-1, keepdims=True)
    )
    return (input_grad.astype(bf16), gate_grad, up_grad, down_grad)


LANE = 128
MESH = pl.DeviceIdType.MESH


class Links:
    def __init__(self, send, recv, local):
        self.send, self.recv, self.local = send, recv, local
        self.names, self.count, self.pending, self.locals = {}, 0, [], 0

    def index(self, name, size=1):
        if name not in self.names:
            self.names[name] = self.count
            self.count += size
        return self.names[name]

    def make(self, name, src, dst, device, size=1, send_at=0, recv_at=0):
        base = self.index(name, size)
        return pltpu.make_async_remote_copy(
            src_ref=src,
            dst_ref=dst,
            send_sem=self.send.at[base + send_at],
            recv_sem=self.recv.at[base + recv_at],
            device_id=device,
            device_id_type=MESH,
        )

    def start(self, name, src, dst, device, when=None, **at):
        copy = self.make(name, src, dst, device, **at)
        guarded(when, copy.start)
        self.pending.append((when, copy))

    def arrive(self, name, dst, device, when=None, **at):
        guarded(when, self.make(name, dst, dst, device, **at).wait_recv)

    def here(self, src, dst, when=None):
        copy = pltpu.make_async_copy(src, dst, self.local.at[self.locals])
        self.locals += 1
        guarded(when, copy.start)
        return lambda: guarded(when, copy.wait)

    def finish(self):
        for when, copy in self.pending:
            guarded(when, copy.wait_send)


def guarded(when, action):
    if when is None:
        action()
    else:
        pl.when(when)(action)


def fused_kernel(
    nz,
    inputs,
    branch,
    cotangent,
    pre_gain,
    post_gain,
    gate,
    up,
    down_w,
    gate_w,
    up_w,
    down_out,
    gate_out,
    up_out,
    rows_out,
    rows,
    acts,
    weights,
    parts,
    near,
    mate,
    side,
    distant,
    tile,
    send,
    recv,
    local,
):
    x, f, c = (lax.axis_index(a) for a in ("rep", "fs", "tp"))
    y, z = lax.rem(f, 2), lax.div(f, 2)
    links = Links(send, recv, local)
    to_x = {"rep": 1 - x}
    to_y = {"fs": f + 1 - 2 * y}
    to_d = {"rep": 1 - x, "fs": f + 1 - 2 * y}
    to_c = {"tp": 1 - c}
    to_up, to_dn = {"fs": f + 2}, {"fs": f - 2}
    has_up, has_dn = z < nz - 1, z > 0

    tokens, model = inputs.shape
    chip = gate.shape[0]
    feats = down_w.shape[0]
    block = 2 * feats
    half = gate.shape[1] // 2
    full = acts.shape[2]
    main = full - LANE
    cut = full // CHUNKS
    tail = CHUNKS - 1
    wide, slim = y == c, y != c
    sources = (down_w, gate_w, up_w)
    outs = (down_out, gate_out, up_out)

    def lanes(start, size):
        return pl.ds(pl.multiple_of(start, LANE), size)

    barrier = pltpu.get_barrier_semaphore()
    for device in (to_x, to_y, to_d, to_c):
        pl.semaphore_signal(barrier, inc=1, device_id=device, device_id_type=MESH)

    @pl.when(has_up)
    def _():
        pl.semaphore_signal(barrier, inc=1, device_id=to_up, device_id_type=MESH)

    @pl.when(has_dn)
    def _():
        pl.semaphore_signal(barrier, inc=1, device_id=to_dn, device_id_type=MESH)

    def own_cols(xx, yy, lo, hi):
        return lanes(xx * half + yy * (main + LANE) + lo, hi - lo)

    def extra_cols(xx):
        return lanes(xx * half + main, LANE)

    my_feats = pl.ds(f * feats, feats)
    own_weight = []
    for w in range(3):
        own_weight.append(
            (
                links.here(
                    sources[w].at[:, own_cols(x, y, 0, main)],
                    weights.at[w, my_feats, pl.ds(0, main)],
                ),
                links.here(
                    sources[w].at[:, extra_cols(x)],
                    weights.at[w, my_feats, pl.ds(main, LANE)],
                    wide,
                ),
            )
        )
    own_acts = []
    for g, saved in ((1, gate), (2, up)):
        own_acts.append(
            links.here(saved.at[:, own_cols(x, y, 0, main)], acts.at[g, pl.ds(0, chip), pl.ds(0, main)])
        )
        own_acts.append(
            links.here(
                saved.at[:, extra_cols(x)], acts.at[g, pl.ds(0, chip), pl.ds(main, LANE)], wide
            )
        )

    def slot_rows(slot, core):
        return pl.ds((slot * 2 + core) * tokens, tokens)

    own_rows = [links.here(v, near.at[i]) for i, v in enumerate((branch, cotangent, inputs))]

    def make_rows(a):
        @pl.loop(0, tokens // 16)
        def _(i):
            at = pl.ds(i * 16, 16)
            v = near[0 if a == 0 else 2, at, :].astype(f32)
            inv = lax.rsqrt(jnp.mean(v * v, axis=-1, keepdims=True) + eps)
            if a == 0:
                u = 0.5 * near[1, at, :].astype(f32) * post_gain[...]
                value = inv * u - v * inv**3 * jnp.mean(u * v, axis=-1, keepdims=True)
            else:
                value = v * inv * pre_gain[...]
            rows[a, pl.ds(c * tokens + i * 16, 16), :] = value.astype(bf16)

    pl.semaphore_wait(barrier, 4 + has_up.astype(jnp.int32) + has_dn.astype(jnp.int32))

    splits = (model, model // 2)

    def row_cols(a, kind):
        first = kind in ("y1", "x2", "x3")
        return pl.ds(0, splits[a]) if first else pl.ds(splits[a], model - splits[a])

    def half_cols(h):
        return pl.ds(h * (model // 2), model // 2)

    def row_send(a, kind):
        device = to_y if kind[0] == "y" else to_x
        relay = {"x3": 1, "y3": 2}
        target = 3 if kind in relay else (1 if kind[0] == "y" else 2)
        source = rows.at[a, slot_rows(relay.get(kind, 0), c), row_cols(a, kind)]
        there = rows.at[a, slot_rows(target, c), row_cols(a, kind)]
        links.start(f"r{a}{kind}", source, there, device)

    def row_wait(a, kind):
        device = to_y if kind[0] == "y" else to_x
        target = 3 if kind in ("x3", "y3") else (1 if kind[0] == "y" else 2)
        links.arrive(f"r{a}{kind}", rows.at[a, slot_rows(target, c), row_cols(a, kind)], device)

    def mate_send(a, slot):
        where = rows.at[a, slot_rows(slot, c), :]
        links.start(f"m{a}{slot}", where, where, to_c)

    def mate_wait(a, slot):
        links.arrive(f"m{a}{slot}", rows.at[a, slot_rows(slot, 1 - c), :], to_c)

    def y_weight(w):
        there = weights.at[w, my_feats, :]
        links.start(
            f"w{w}y",
            sources[w].at[:, own_cols(x, 1 - y, 0, main)],
            there.at[:, pl.ds(0, main)],
            to_y,
        )
        links.start(
            f"w{w}e", sources[w].at[:, extra_cols(x)], there.at[:, pl.ds(main, LANE)], to_y, slim
        )

    def y_weight_wait(w):
        there = weights.at[w, pl.ds((f + 1 - 2 * y) * feats, feats), :]
        links.arrive(f"w{w}y", there.at[:, pl.ds(0, main)], to_y)
        links.arrive(f"w{w}e", there.at[:, pl.ds(main, LANE)], to_y, wide)

    def weight_piece(w, origin, o, width):
        yy = y if o == 0 else 1 - y
        return weights.at[w, pl.ds((origin * 2 + yy) * feats, feats), pl.ds(0, width)]

    def z_send(w, o, hop):
        for width, size in ((full, wide), (main, slim)):
            ahead = weight_piece(w, jnp.maximum(z - hop, 0), o, width)
            when = size & has_up & (z >= hop)
            links.start(f"z{w}{o}u{hop}", ahead, ahead, to_up, when)
            behind = weight_piece(w, jnp.minimum(z + hop, nz - 1), o, width)
            when = size & has_dn & (z + hop < nz)
            links.start(f"z{w}{o}d{hop}", behind, behind, to_dn, when)

    def z_wait(w, o, hop, here):
        for width, size in ((full, wide & here), (main, slim & here)):
            ahead = weight_piece(w, jnp.maximum(z - hop, 0), o, width)
            links.arrive(f"z{w}{o}u{hop - 1}", ahead, to_up, size & (z >= hop))
            behind = weight_piece(w, jnp.minimum(z + hop, nz - 1), o, width)
            links.arrive(f"z{w}{o}d{hop - 1}", behind, to_dn, size & (z + hop < nz))

    ends = (z == 0) | (z == nz - 1)
    inner = jnp.logical_not(ends)

    def z_step(w, o, hop):
        z_wait(w, o, hop, inner)
        z_send(w, o, hop)

    def z_rest(w):
        for o in range(2):
            for hop in range(1, nz - 1):
                z_wait(w, o, hop, ends)
            z_wait(w, o, nz - 1, ends | inner)

    peers = ((2, to_x, 1 - x, y), (1, to_y, x, 1 - y), (3, to_d, 1 - x, 1 - y))

    def act_send(q, slots):
        for slot, device, xx, yy in peers:
            if slot not in slots:
                continue
            for g, saved in ((1, gate), (2, up)):
                there = acts.at[g, pl.ds(slot * chip, chip), :]
                lo, hi = q * cut, min((q + 1) * cut, main)
                links.start(
                    f"a{q}{g}{slot}",
                    saved.at[:, own_cols(xx, yy, lo, hi)],
                    there.at[:, pl.ds(lo, hi - lo)],
                    device,
                )
                if q == tail:
                    links.start(
                        f"e{g}{slot}",
                        saved.at[:, extra_cols(xx)],
                        there.at[:, pl.ds(main, LANE)],
                        device,
                        yy == c,
                    )

    def act_wait(q):
        for slot, device, _, _ in peers:
            for g in (1, 2):
                there = acts.at[g, pl.ds(slot * chip, chip), :]
                lo, hi = q * cut, min((q + 1) * cut, main)
                links.arrive(f"a{q}{g}{slot}", there.at[:, pl.ds(lo, hi - lo)], device)
                if q == tail:
                    links.arrive(f"e{g}{slot}", there.at[:, pl.ds(main, LANE)], device, wide)

    total = acts.shape[1]

    def make_hidden(q):
        cols = pl.ds(q * cut, cut)

        @pl.loop(0, total // 64)
        def _(i):
            at = pl.ds(i * 64, 64)
            g = acts[1, at, cols].astype(f32)
            u = acts[2, at, cols].astype(f32)
            acts[0, at, cols] = (g * jax.nn.sigmoid(g) * u).astype(bf16)

    def make_cots(q):
        cols = pl.ds(q * cut, cut)

        @pl.loop(0, total // 256)
        def _(i):
            at = pl.ds(i * 256, 256)
            tile[pl.ds(0, 256), :] = jnp.dot(
                rows[0, at, :], weights[0, :, cols], preferred_element_type=f32
            )

            @pl.loop(0, 4)
            def _(j):
                sub = pl.ds(i * 256 + j * 64, 64)
                grad = tile[pl.ds(j * 64, 64), :]
                g = acts[1, sub, cols].astype(f32)
                u = acts[2, sub, cols].astype(f32)
                s = jax.nn.sigmoid(g)
                acts[1, sub, cols] = (grad * u * s * (1.0 + g * (1.0 - s))).astype(bf16)
                acts[2, sub, cols] = (grad * (g * s)).astype(bf16)

    def order(s):
        def low(zz):
            return jnp.where(
                s < nz - 1 - zz, nz - 1 - s, jnp.where(s == nz - 1, zz, s - (nz - 1 - zz))
            )

        return jnp.where(2 * z < nz, low(z), nz - 1 - low(nz - 1 - z))

    def grad_step(q, g, s):
        d = order(s)
        cols = lanes(q * cut, cut)

        @pl.loop(0, block // 256)
        def _(m):
            tile[pl.ds(m * 256, 256), :] = contract_rows(
                rows[jnp.minimum(g, 1), :, pl.ds(pl.multiple_of(d * block + m * 256, 256), 256)],
                acts[g, :, cols],
            )

        sizes = ((cut, (q < tail) | wide), (cut - LANE, (q == tail) & slim))
        spot = (q * 3 + g) * (nz + 1)
        count = 3 * CHUNKS * (nz + 1)

        def take(slot, when):
            for width, size in sizes:
                links.arrive(
                    "p",
                    parts.at[g, slot, :, lanes(q * cut, width)],
                    to_up,
                    when & size,
                    size=count,
                    recv_at=spot + slot,
                )

        far = d != z
        fed = jnp.where(d > z, has_dn, jnp.where(d < z, has_up, has_dn))
        take(d, fed)

        @pl.loop(0, block // 64)
        def _(i):
            at = pl.ds(i * 64, 64)

            @pl.when(fed)
            def _():
                tile[at, :] += parts[g, d, at, cols].astype(f32)

        take(nz, (d == z) & has_up)

        @pl.when((d == z) & has_up)
        def _():
            @pl.loop(0, block // 64)
            def _(i):
                at = pl.ds(i * 64, 64)
                tile[at, :] += parts[g, nz, at, cols].astype(f32)

        @pl.loop(0, block // 64)
        def _(i):
            at = pl.ds(i * 64, 64)
            parts[g, d, at, cols] = tile[at, :].astype(bf16)

        target = jnp.where(d == z - 1, nz, d)
        device = {"fs": jnp.where(d > z, f + 2, f - 2)}
        for width, size in sizes:
            copy = links.make(
                "p",
                parts.at[g, d, :, lanes(q * cut, width)],
                parts.at[g, target, :, lanes(q * cut, width)],
                device,
                size=count,
                send_at=spot + d,
                recv_at=spot + target,
            )
            guarded(far & size, copy.start)

    def grad_sent():
        @pl.loop(0, 3 * CHUNKS)
        def _(i):
            q, g = lax.div(i, 3), lax.rem(i, 3)
            spot = i * (nz + 1)

            @pl.loop(0, nz)
            def _(d):
                for width, size in (
                    (cut, (q < tail) | wide),
                    (cut - LANE, (q == tail) & slim),
                ):
                    copy = links.make(
                        "p",
                        parts.at[g, d, :, lanes(q * cut, width)],
                        parts.at[g, d, :, lanes(q * cut, width)],
                        to_up,
                        send_at=spot + d,
                        recv_at=spot + d,
                    )
                    guarded((d != z) & size, copy.wait_send)

    out_waits = []

    def spread(q, g):
        lo, hi = q * cut, min((q + 1) * cut, main)
        pieces = [("o", lo, hi - lo, y * (main + LANE) + lo, (1 - y) * (main + LANE) + lo, None)]
        if q == tail:
            pieces.append(("e", main, LANE, main, main, wide))
        keep = parts.at[g, z, pl.ds(y * feats, feats), :]
        give = parts.at[g, z, pl.ds((1 - y) * feats, feats), :]
        for tag, start, size, here, other, when in pieces:
            name = f"h{q}{g}{tag}"
            there = outs[g].at[:, lanes(x * half + here, size)]
            out_waits.append(links.here(keep.at[:, pl.ds(start, size)], there, when))
            far_side = [(to_x, 1 - x, here, when), (to_y, x, other, slim), (to_d, 1 - x, other, slim)]
            for i, (device, xx, col, back_when) in enumerate(far_side):
                source = keep if i == 0 else give
                links.start(f"{name}{i}", source.at[:, pl.ds(start, size)], there, device, when)
                back = outs[g].at[:, lanes(xx * half + col, size)]
                back_when = None if when is None else back_when
                out_waits.append(
                    functools.partial(links.arrive, f"{name}{i}", back, device, back_when)
                )

    def turn(i):
        return jnp.where(i < 2, 3 - 2 * i, 6 - 2 * i)

    def row_grad(core, slot, target, add):
        at = pl.ds((slot * 2 + core) * tokens, tokens)

        @pl.loop(0, 4)
        def _(n):
            wide_cols = lanes(n * (model // 4), model // 4)
            feat_rows = pl.ds(n * (model // 4), model // 4)
            value = contract_cols(acts[1, at, :], weights[1, feat_rows, :])
            value = value + contract_cols(acts[2, at, :], weights[2, feat_rows, :])
            if add:
                value = value + mate[slot, :, wide_cols].astype(f32)
            target[slot, :, wide_cols] = value.astype(bf16)

    def to_mate(slot):
        return links.make(
            "s", near.at[slot], mate.at[slot], to_c, size=4, send_at=slot, recv_at=slot
        )

    def rows_for_mate(lo, hi):
        @pl.loop(lo, hi)
        def _(i):
            slot = turn(i)
            row_grad(1 - c, slot, near, False)
            to_mate(slot).start()

    def rows_here(lo, hi):
        @pl.loop(lo, hi)
        def _(i):
            slot = turn(i)
            to_mate(slot).wait_recv()
            row_grad(c, slot, mate, True)

    def pass_on(slot, h):
        device, at = (to_y, slot // 2) if h == 0 else (to_x, slot % 2)
        links.start(
            f"t{slot}{h}", mate.at[slot, :, half_cols(h)], side.at[at, :, half_cols(h)], device
        )

    def gather_in(slot, h, last):
        there = slot + (1 if h == 0 else 2)
        device, at = (to_y, there // 2) if h == 0 else (to_x, there % 2)
        links.arrive(f"t{there}{h}", side.at[at, :, half_cols(h)], device)

        @pl.loop(0, tokens // 32)
        def _(i):
            r = pl.ds(i * 32, 32)
            value = mate[slot, r, half_cols(h)].astype(f32) + side[at, r, half_cols(h)].astype(f32)
            mate[slot, r, half_cols(h)] = value.astype(bf16)

        if not last:
            device = to_x if h == 0 else to_y
            there = distant.at[:, half_cols(h)]
            links.start(f"u{h}", mate.at[slot, :, half_cols(h)], there, device)

    def reload():
        @pl.loop(0, 4)
        def _(slot):
            to_mate(slot).wait_send()

        return [links.here(v, near.at[i]) for i, v in ((1, cotangent), (2, inputs))]

    def finish_rows(waits):
        for wait in waits:
            wait()
        for h in range(2):
            device = to_x if h == 0 else to_y
            links.arrive(f"u{h}", distant.at[:, half_cols(h)], device)

        @pl.loop(0, tokens // 16)
        def _(i):
            at = pl.ds(i * 16, 16)
            grad = mate[0, at, :].astype(f32) + distant[at, :].astype(f32)
            v = near[2, at, :].astype(f32)
            inv = lax.rsqrt(jnp.mean(v * v, axis=-1, keepdims=True) + eps)
            w = grad * pre_gain[...]
            value = near[1, at, :].astype(f32) + inv * w
            value = value - v * inv**3 * jnp.mean(w * v, axis=-1, keepdims=True)
            near[0, at, :] = value.astype(bf16)

        out_waits.append(links.here(near.at[0], rows_out))

    last = nz - 1

    def run(q, g, s, count, when=None):
        @pl.loop(0, count if when is None else jnp.where(when, count, 0))
        def _(i):
            k = s + i
            grad_step(q, g + lax.div(k, last), lax.rem(k, last))

    def close(q, g):
        grad_step(q, g, last)
        spread(q, g)

    y_weight(0)
    act_send(0, (2,))
    for wait in own_weight[0]:
        wait()
    z_send(0, 0, 0)
    for wait in own_rows:
        wait()
    make_rows(0)
    row_send(0, "y1")
    row_send(0, "x2")
    y_weight(1)
    y_weight(2)
    act_send(0, (1,))
    mate_send(0, 0)
    make_rows(1)
    mate_send(1, 0)
    y_weight_wait(0)
    z_send(0, 1, 0)

    @pl.when(slim)
    def _():
        @pl.loop(0, total // 64)
        def _(i):
            at = pl.ds(i * 64, 64)
            for g in (1, 2):
                acts[g, at, pl.ds(main, LANE)] = jnp.zeros((64, LANE), bf16)

        @pl.loop(0, model // 64)
        def _(i):
            at = pl.ds(i * 64, 64)
            for w in range(3):
                weights[w, at, pl.ds(main, LANE)] = jnp.zeros((64, LANE), bf16)

    z_step(0, 0, 1)
    z_step(0, 1, 1)
    row_wait(0, "y1")
    row_send(0, "x3")
    act_send(0, (3,))
    for kind in ("y1", "x1", "x2", "y2"):
        row_send(1, kind)
    mate_send(0, 1)
    for hop in range(2, last):
        z_step(0, 0, hop)
        z_step(0, 1, hop)
    for w in (1, 2):
        for wait in own_weight[w]:
            wait()
        z_send(w, 0, 0)
    row_wait(0, "x2")
    mate_send(0, 2)
    for w in (1, 2):
        y_weight_wait(w)
        z_send(w, 1, 0)
    row_wait(0, "x3")
    mate_send(0, 3)
    for o in range(2):
        for w in (1, 2):
            z_step(w, o, 1)
    for wait in own_acts:
        wait()
    act_wait(0)
    make_hidden(0)
    for slot in range(4):
        mate_wait(0, slot)
    run(0, 0, 0, 1)
    row_wait(1, "x1")
    row_send(1, "y3")
    row_wait(1, "y1")
    row_send(1, "x3")
    act_send(1, (1, 2, 3))
    act_send(2, (1, 2, 3))
    for hop in range(2, last):
        for w in (1, 2):
            z_step(w, 0, hop)
    run(0, 0, 1, 1)
    z_rest(0)
    make_cots(0)
    run(0, 0, 2, last - 2)
    row_wait(1, "y2")
    mate_send(1, 1)
    row_wait(1, "x2")
    mate_send(1, 2)
    for hop in range(2, last):
        for w in (1, 2):
            z_step(w, 1, hop)
    row_wait(1, "x3")
    row_wait(1, "y3")
    mate_send(1, 3)
    for slot in range(4):
        mate_wait(1, slot)
    run(0, 1, 0, last)
    run(0, 2, 0, 1)
    run(0, 2, 1, last - 1, ends)
    act_wait(1)
    make_hidden(1)
    make_cots(1)
    run(1, 0, 0, 3 * last, ends)
    run(0, 2, 1, last - 1, inner)
    act_wait(2)
    make_hidden(2)
    make_cots(2)
    run(2, 0, 0, 3 * last, ends)
    run(1, 0, 0, last, inner)
    for g in range(3):
        close(0, g)
    z_rest(1)
    z_rest(2)
    rows_for_mate(0, 4)
    run(1, 1, 0, last, inner)
    close(1, 0)
    rows_here(0, 2)
    pass_on(3, 0)
    pass_on(3, 1)
    pass_on(1, 0)
    rows_here(2, 4)
    pass_on(2, 1)
    run(1, 2, 0, last, inner)
    again = reload()
    close(1, 1)
    run(2, 0, 0, last, inner)
    gather_in(2, 0, False)
    gather_in(1, 1, False)
    close(1, 2)
    run(2, 1, 0, last, inner)
    gather_in(0, 0, True)
    gather_in(0, 1, True)
    close(2, 0)
    run(2, 2, 0, 2, inner)
    finish_rows(again)
    close(2, 1)
    run(2, 2, 2, last - 2, inner)
    close(2, 2)
    for wait in out_waits:
        wait()
    grad_sent()
    links.finish()


def fused_device(nz, block_input, pre_gain, post_gain, gate_saved, up_saved, branch_saved,
                 out_cotangent, gate_weight, up_weight, down_weight):
    tokens, model = block_input.shape
    chip, width = gate_saved.shape
    feats = down_weight.shape[0]
    full = (width // 2 // LANE + 1) // 2 * LANE
    grad = jax.ShapeDtypeStruct((feats, width), bf16)
    total = jax.ShapeDtypeStruct((tokens, model), bf16)
    down_grad, gate_grad, up_grad, input_grad = pl.pallas_call(
        functools.partial(fused_kernel, nz),
        out_shape=(grad, grad, grad, total),
        in_specs=[pl.BlockSpec(memory_space=pl.ANY)] * 3
        + [pl.BlockSpec(memory_space=pltpu.VMEM)] * 2
        + [pl.BlockSpec(memory_space=pl.ANY)] * 5,
        out_specs=[pl.BlockSpec(memory_space=pl.ANY)] * 4,
        scratch_shapes=[
            pltpu.VMEM((2, 4 * chip, model), bf16),
            pltpu.VMEM((3, 4 * chip, full), bf16),
            pltpu.VMEM((3, model, full), bf16),
            pltpu.VMEM((3, nz + 1, 2 * feats, full), bf16),
            pltpu.VMEM((4, tokens, model), bf16),
            pltpu.VMEM((4, tokens, model), bf16),
            pltpu.VMEM((2, tokens, model), bf16),
            pltpu.VMEM((tokens, model), bf16),
            pltpu.VMEM((2 * feats, full // CHUNKS), f32),
            pltpu.SemaphoreType.DMA((SEMS,)),
            pltpu.SemaphoreType.DMA((SEMS,)),
            pltpu.SemaphoreType.DMA((LOCALS,)),
        ],
        compiler_params=pltpu.CompilerParams(
            collective_id=0, has_side_effects=True, vmem_limit_bytes=66_900_000
        ),
    )(
        block_input,
        branch_saved,
        out_cotangent,
        pre_gain.reshape(1, model),
        post_gain.reshape(1, model),
        gate_saved,
        up_saved,
        down_weight,
        gate_weight,
        up_weight,
    )

    return (
        input_grad,
        gate_grad.astype(f32),
        up_grad.astype(f32),
        down_grad.astype(f32),
    )


def solution(mesh):
    shape = mesh.shape

    def run(*args):
        width = args[3].shape[1] // shape["tp"]
        tiles, odd = divmod(width // 2, LANE)
        fits = shape["rep"] == 2 and shape["tp"] == 2 and shape["fs"] % 2 == 0
        fits = fits and width % 2 == 0 and odd == 0 and tiles % 6 == 5
        if fits:
            per_device = functools.partial(fused_device, shape["fs"] // 2)
        else:
            per_device = functools.partial(plain_device, shape["rep"])
        return jax.shard_map(
            per_device,
            mesh=mesh,
            in_specs=(
                P(("rep", "fs", "tp"), None),
                P(),
                P(),
                P(("rep", "fs"), "tp"),
                P(("rep", "fs"), "tp"),
                P(("rep", "fs", "tp"), None),
                P(("rep", "fs", "tp"), None),
                P("fs", "tp"),
                P("fs", "tp"),
                P("fs", "tp"),
            ),
            out_specs=(P(("rep", "fs", "tp"), None), P("fs", "tp"), P("fs", "tp"), P("fs", "tp")),
            check_vma=False,
        )(*args)

    return run
```

```python
import functools

import jax
import jax.numpy as jnp
from jax import lax
from jax.experimental import pallas as pl
from jax.experimental.pallas import tpu as pltpu
from jax.sharding import PartitionSpec as P

eps = 1e-06
bf16, f32 = jnp.bfloat16, jnp.float32
SEMS, LOCALS = 240, 64
CHUNKS = 3
LINE = 4


def contract_rows(left, right):
    return lax.dot_general(
        left, right, (((0,), (0,)), ((), ())), preferred_element_type=jnp.float32
    )


def contract_cols(left, right):
    return lax.dot_general(
        left, right, (((1,), (1,)), ((), ())), preferred_element_type=jnp.float32
    )


def shifted(value, reps, step):
    return lax.ppermute(value, "rep", [(i, (i + step) % reps) for i in range(reps)])


def plain_device(
    reps,
    block_input,
    pre_gain,
    post_gain,
    gate_saved,
    up_saved,
    branch_saved,
    out_cotangent,
    gate_weight,
    up_weight,
    down_weight,
):
    me = lax.axis_index("rep")
    width = gate_saved.shape[1] // reps

    def columns(value, owner):
        return lax.dynamic_slice_in_dim(value, owner * width, width, axis=1)

    down_full = lax.all_gather(columns(down_weight, me), "fs", axis=0, tiled=True)

    gates = [columns(gate_saved, me)]
    ups = [columns(up_saved, me)]
    for k in range(1, reps):
        there = lax.rem(me + k, reps)
        gates.append(shifted(columns(gate_saved, there), reps, k))
        ups.append(shifted(columns(up_saved, there), reps, k))

    xfull = block_input.astype(f32)
    inv_x = lax.rsqrt(jnp.mean(xfull * xfull, axis=-1, keepdims=True) + eps)
    normed = (xfull * inv_x * pre_gain).astype(bf16)
    branch = branch_saved.astype(f32)
    inv_b = lax.rsqrt(jnp.mean(branch * branch, axis=-1, keepdims=True) + eps)
    upstream = 0.5 * out_cotangent.astype(f32) * post_gain
    branch_grad = (
        inv_b * upstream - branch * inv_b**3 * jnp.mean(upstream * branch, axis=-1, keepdims=True)
    ).astype(bf16)

    normed_own = [normed] + [shifted(normed, reps, k) for k in range(1, reps)]
    branch_own = [branch_grad] + [shifted(branch_grad, reps, k) for k in range(1, reps)]
    normed_rows = [lax.all_gather(v, "tp", axis=0, tiled=True) for v in normed_own]
    branch_rows = [lax.all_gather(v, "tp", axis=0, tiled=True) for v in branch_own]
    normed_all = jnp.concatenate(normed_rows, axis=0)
    branch_all = jnp.concatenate(branch_rows, axis=0)

    gate_f = jnp.concatenate(gates, axis=0).astype(f32)
    up_f = jnp.concatenate(ups, axis=0).astype(f32)
    sigma = jax.nn.sigmoid(gate_f)
    silu_gate = gate_f * sigma
    hidden = (silu_gate * up_f).astype(bf16)

    def spread(total):
        shard = lax.psum_scatter(total.astype(bf16), "fs", scatter_dimension=0, tiled=True)
        out = jnp.zeros((shard.shape[0], width * reps), f32)
        out = lax.dynamic_update_slice_in_dim(out, shard.astype(f32), me * width, axis=1)
        for k in range(1, reps):
            other = shifted(shard, reps, k).astype(f32)
            out = lax.dynamic_update_slice_in_dim(
                out, other, lax.rem(me - k + reps, reps) * width, axis=1
            )
        return out

    down_grad = spread(contract_rows(branch_all, hidden))

    hidden_grad = jnp.dot(branch_all, down_full, preferred_element_type=f32)
    gate_cot = (hidden_grad * up_f * sigma * (1.0 + gate_f * (1.0 - sigma))).astype(bf16)
    up_cot = (hidden_grad * silu_gate).astype(bf16)
    gate_grad = spread(contract_rows(normed_all, gate_cot))
    up_grad = spread(contract_rows(normed_all, up_cot))

    gate_full = lax.all_gather(columns(gate_weight, me), "fs", axis=0, tiled=True)
    up_full = lax.all_gather(columns(up_weight, me), "fs", axis=0, tiled=True)
    partial = (contract_cols(gate_cot, gate_full) + contract_cols(up_cot, up_full)).astype(bf16)
    rows = partial.shape[0] // reps
    normed_grad = None
    for k in range(reps):
        piece = lax.psum_scatter(
            partial[k * rows : (k + 1) * rows], "tp", scatter_dimension=0, tiled=True
        )
        if k:
            piece = shifted(piece, reps, reps - k)
        piece = piece.astype(f32)
        normed_grad = piece if normed_grad is None else normed_grad + piece

    scaled = normed_grad * pre_gain
    input_grad = (
        out_cotangent.astype(f32)
        + inv_x * scaled
        - xfull * inv_x**3 * jnp.mean(scaled * xfull, axis=-1, keepdims=True)
    )
    return (input_grad.astype(bf16), gate_grad, up_grad, down_grad)


LANE = 128
MESH = pl.DeviceIdType.MESH


class Links:
    def __init__(self, send, recv, local):
        self.send, self.recv, self.local = send, recv, local
        self.names, self.count, self.pending, self.locals = {}, 0, [], 0

    def index(self, name, size=1):
        if name not in self.names:
            self.names[name] = self.count
            self.count += size
        return self.names[name]

    def make(self, name, src, dst, device, size=1, send_at=0, recv_at=0):
        base = self.index(name, size)
        return pltpu.make_async_remote_copy(
            src_ref=src,
            dst_ref=dst,
            send_sem=self.send.at[base + send_at],
            recv_sem=self.recv.at[base + recv_at],
            device_id=device,
            device_id_type=MESH,
        )

    def start(self, name, src, dst, device, when=None, **at):
        copy = self.make(name, src, dst, device, **at)
        guarded(when, copy.start)
        self.pending.append((when, copy))

    def arrive(self, name, dst, device, when=None, **at):
        guarded(when, self.make(name, dst, dst, device, **at).wait_recv)

    def here(self, src, dst, when=None):
        copy = pltpu.make_async_copy(src, dst, self.local.at[self.locals])
        self.locals += 1
        guarded(when, copy.start)
        return lambda: guarded(when, copy.wait)

    def finish(self):
        for when, copy in self.pending:
            guarded(when, copy.wait_send)


def guarded(when, action):
    if when is None:
        action()
    else:
        pl.when(when)(action)


def fused_kernel(
    nz,
    inputs,
    branch,
    cotangent,
    pre_gain,
    post_gain,
    gate,
    up,
    down_w,
    gate_w,
    up_w,
    down_out,
    gate_out,
    up_out,
    rows_out,
    rows,
    acts,
    weights,
    parts,
    near,
    mate,
    side,
    distant,
    tile,
    send,
    recv,
    local,
):
    x, f, c = (lax.axis_index(a) for a in ("rep", "fs", "tp"))
    y, z = lax.rem(f, 2), lax.div(f, 2)
    links = Links(send, recv, local)
    to_x = {"rep": 1 - x}
    to_y = {"fs": f + 1 - 2 * y}
    to_d = {"rep": 1 - x, "fs": f + 1 - 2 * y}
    to_c = {"tp": 1 - c}
    to_up, to_dn = {"fs": f + 2}, {"fs": f - 2}
    has_up, has_dn = z < nz - 1, z > 0

    tokens, model = inputs.shape
    chip = gate.shape[0]
    feats = down_w.shape[0]
    block = 2 * feats
    half = gate.shape[1] // 2
    full = acts.shape[2]
    main = full - LANE
    cut = full // CHUNKS
    tail = CHUNKS - 1
    wide, slim = y == c, y != c
    sources = (down_w, gate_w, up_w)
    outs = (down_out, gate_out, up_out)

    def lanes(start, size):
        return pl.ds(pl.multiple_of(start, LANE), size)

    barrier = pltpu.get_barrier_semaphore()
    for device in (to_x, to_y, to_d, to_c):
        pl.semaphore_signal(barrier, inc=1, device_id=device, device_id_type=MESH)

    @pl.when(has_up)
    def _():
        pl.semaphore_signal(barrier, inc=1, device_id=to_up, device_id_type=MESH)

    @pl.when(has_dn)
    def _():
        pl.semaphore_signal(barrier, inc=1, device_id=to_dn, device_id_type=MESH)

    def own_cols(xx, yy, lo, hi):
        return lanes(xx * half + yy * (main + LANE) + lo, hi - lo)

    def extra_cols(xx):
        return lanes(xx * half + main, LANE)

    my_feats = pl.ds(f * feats, feats)
    own_weight = []
    for w in range(3):
        own_weight.append(
            (
                links.here(
                    sources[w].at[:, own_cols(x, y, 0, main)],
                    weights.at[w, my_feats, pl.ds(0, main)],
                ),
                links.here(
                    sources[w].at[:, extra_cols(x)],
                    weights.at[w, my_feats, pl.ds(main, LANE)],
                    wide,
                ),
            )
        )
    own_acts = []
    for g, saved in ((1, gate), (2, up)):
        own_acts.append(
            links.here(saved.at[:, own_cols(x, y, 0, main)], acts.at[g, pl.ds(0, chip), pl.ds(0, main)])
        )
        own_acts.append(
            links.here(
                saved.at[:, extra_cols(x)], acts.at[g, pl.ds(0, chip), pl.ds(main, LANE)], wide
            )
        )

    def slot_rows(slot, core):
        return pl.ds((slot * 2 + core) * tokens, tokens)

    own_rows = [links.here(v, near.at[i]) for i, v in enumerate((branch, cotangent, inputs))]

    def make_rows(a):
        @pl.loop(0, tokens // 16)
        def _(i):
            at = pl.ds(i * 16, 16)
            v = near[0 if a == 0 else 2, at, :].astype(f32)
            inv = lax.rsqrt(jnp.mean(v * v, axis=-1, keepdims=True) + eps)
            if a == 0:
                u = 0.5 * near[1, at, :].astype(f32) * post_gain[...]
                value = inv * u - v * inv**3 * jnp.mean(u * v, axis=-1, keepdims=True)
            else:
                value = v * inv * pre_gain[...]
            rows[a, pl.ds(c * tokens + i * 16, 16), :] = value.astype(bf16)

        for k in range(nz):
            mate_send(a, k, 0)

    pl.semaphore_wait(barrier, 4 + has_up.astype(jnp.int32) + has_dn.astype(jnp.int32))

    def order(s):
        def low(zz):
            return jnp.where(
                s < nz - 1 - zz, nz - 1 - s, jnp.where(s == nz - 1, zz, s - (nz - 1 - zz))
            )

        return jnp.where(2 * z < nz, low(z), nz - 1 - low(nz - 1 - z))

    routes = (("y", "y", "y", "y"), ("x", "y", "x", "y"))

    def half_cols(h):
        return pl.ds(h * (model // 2), model // 2)

    def row_part(a, k, slot, core):
        return rows.at[a, slot_rows(slot, core), lanes(order(k) * block, block)]

    def row_path(a, k):
        y_way, x_way = (to_y, 1), (to_x, 2)
        return (y_way, x_way) if routes[a][k] == "y" else (x_way, y_way)

    def row_first(a, k):
        (device, slot), _ = row_path(a, k)
        links.start(f"f{a}{k}", row_part(a, k, 0, c), row_part(a, k, slot, c), device)

    def row_other(a, k):
        _, (device, slot) = row_path(a, k)
        links.start(f"o{a}{k}", row_part(a, k, 0, c), row_part(a, k, slot, c), device)

    def row_relay(a, k):
        (device, slot), (onward, _) = row_path(a, k)
        links.arrive(f"f{a}{k}", row_part(a, k, slot, c), device)
        links.start(f"r{a}{k}", row_part(a, k, slot, c), row_part(a, k, 3, c), onward)
        mate_send(a, k, slot)

    def row_other_in(a, k):
        _, (device, slot) = row_path(a, k)
        links.arrive(f"o{a}{k}", row_part(a, k, slot, c), device)
        mate_send(a, k, slot)

    def row_last_in(a, k):
        _, (onward, _) = row_path(a, k)
        links.arrive(f"r{a}{k}", row_part(a, k, 3, c), onward)
        mate_send(a, k, 3)

    def mate_send(a, k, slot):
        links.start(f"m{a}{k}{slot}", row_part(a, k, slot, c), row_part(a, k, slot, c), to_c)

    def row_ready(a, k):
        for slot in range(4):
            links.arrive(f"m{a}{k}{slot}", row_part(a, k, slot, 1 - c), to_c)

    def y_weight(w):
        there = weights.at[w, my_feats, :]
        links.start(
            f"w{w}y",
            sources[w].at[:, own_cols(x, 1 - y, 0, main)],
            there.at[:, pl.ds(0, main)],
            to_y,
        )
        links.start(
            f"w{w}e", sources[w].at[:, extra_cols(x)], there.at[:, pl.ds(main, LANE)], to_y, slim
        )

    def y_weight_wait(w):
        there = weights.at[w, pl.ds((f + 1 - 2 * y) * feats, feats), :]
        links.arrive(f"w{w}y", there.at[:, pl.ds(0, main)], to_y)
        links.arrive(f"w{w}e", there.at[:, pl.ds(main, LANE)], to_y, wide)

    def weight_piece(w, origin, o, width):
        yy = y if o == 0 else 1 - y
        return weights.at[w, pl.ds((origin * 2 + yy) * feats, feats), pl.ds(0, width)]

    def z_send(w, o, hop):
        for width, size in ((full, wide), (main, slim)):
            ahead = weight_piece(w, jnp.maximum(z - hop, 0), o, width)
            when = size & has_up & (z >= hop)
            links.start(f"z{w}{o}u{hop}", ahead, ahead, to_up, when)
            behind = weight_piece(w, jnp.minimum(z + hop, nz - 1), o, width)
            when = size & has_dn & (z + hop < nz)
            links.start(f"z{w}{o}d{hop}", behind, behind, to_dn, when)

    def z_wait(w, o, hop, here):
        for width, size in ((full, wide & here), (main, slim & here)):
            ahead = weight_piece(w, jnp.maximum(z - hop, 0), o, width)
            links.arrive(f"z{w}{o}u{hop - 1}", ahead, to_up, size & (z >= hop))
            behind = weight_piece(w, jnp.minimum(z + hop, nz - 1), o, width)
            links.arrive(f"z{w}{o}d{hop - 1}", behind, to_dn, size & (z + hop < nz))

    ends = (z == 0) | (z == nz - 1)
    inner = jnp.logical_not(ends)

    def z_step(w, o, hop):
        z_wait(w, o, hop, inner)
        z_send(w, o, hop)

    def z_rest(w):
        for o in range(2):
            for hop in range(1, nz - 1):
                z_wait(w, o, hop, ends)
            z_wait(w, o, nz - 1, ends | inner)

    peers = ((2, to_x, 1 - x, y), (1, to_y, x, 1 - y), (3, to_d, 1 - x, 1 - y))

    def act_send(q, to):
        for slot, device, xx, yy in peers:
            if slot != to:
                continue
            for g, saved in ((1, gate), (2, up)):
                there = acts.at[g, pl.ds(slot * chip, chip), :]
                lo, hi = q * cut, min((q + 1) * cut, main)
                links.start(
                    f"a{q}{g}{slot}",
                    saved.at[:, own_cols(xx, yy, lo, hi)],
                    there.at[:, pl.ds(lo, hi - lo)],
                    device,
                )
                if q == tail:
                    links.start(
                        f"e{g}{slot}",
                        saved.at[:, extra_cols(xx)],
                        there.at[:, pl.ds(main, LANE)],
                        device,
                        yy == c,
                    )

    def act_wait(q):
        for slot, device, _, _ in peers:
            for g in (1, 2):
                there = acts.at[g, pl.ds(slot * chip, chip), :]
                lo, hi = q * cut, min((q + 1) * cut, main)
                links.arrive(f"a{q}{g}{slot}", there.at[:, pl.ds(lo, hi - lo)], device)
                if q == tail:
                    links.arrive(f"e{g}{slot}", there.at[:, pl.ds(main, LANE)], device, wide)

    total = acts.shape[1]

    def make_hidden(q):
        cols = pl.ds(q * cut, cut)

        @pl.loop(0, total // 64)
        def _(i):
            at = pl.ds(i * 64, 64)
            g = acts[1, at, cols].astype(f32)
            u = acts[2, at, cols].astype(f32)
            acts[0, at, cols] = (g * jax.nn.sigmoid(g) * u).astype(bf16)

    def make_cots(q):
        cols = pl.ds(q * cut, cut)

        @pl.loop(0, total // 256)
        def _(i):
            at = pl.ds(i * 256, 256)
            tile[pl.ds(0, 256), :] = jnp.dot(
                rows[0, at, :], weights[0, :, cols], preferred_element_type=f32
            )

            @pl.loop(0, 4)
            def _(j):
                sub = pl.ds(i * 256 + j * 64, 64)
                grad = tile[pl.ds(j * 64, 64), :]
                g = acts[1, sub, cols].astype(f32)
                u = acts[2, sub, cols].astype(f32)
                s = jax.nn.sigmoid(g)
                acts[1, sub, cols] = (grad * u * s * (1.0 + g * (1.0 - s))).astype(bf16)
                acts[2, sub, cols] = (grad * (g * s)).astype(bf16)

    def grad_step(q, g, s):
        d = order(s)
        cols = lanes(q * cut, cut)

        @pl.loop(0, block // 256)
        def _(m):
            tile[pl.ds(m * 256, 256), :] = contract_rows(
                rows[jnp.minimum(g, 1), :, pl.ds(pl.multiple_of(d * block + m * 256, 256), 256)],
                acts[g, :, cols],
            )

        sizes = ((cut, (q < tail) | wide), (cut - LANE, (q == tail) & slim))
        spot = (q * 3 + g) * (nz + 1)
        count = 3 * CHUNKS * (nz + 1)

        def take(slot, when):
            for width, size in sizes:
                links.arrive(
                    "p",
                    parts.at[g, slot, :, lanes(q * cut, width)],
                    to_up,
                    when & size,
                    size=count,
                    recv_at=spot + slot,
                )

        far = d != z
        fed = jnp.where(d > z, has_dn, jnp.where(d < z, has_up, has_dn))
        take(d, fed)

        @pl.loop(0, block // 64)
        def _(i):
            at = pl.ds(i * 64, 64)

            @pl.when(fed)
            def _():
                tile[at, :] += parts[g, d, at, cols].astype(f32)

        take(nz, (d == z) & has_up)

        @pl.when((d == z) & has_up)
        def _():
            @pl.loop(0, block // 64)
            def _(i):
                at = pl.ds(i * 64, 64)
                tile[at, :] += parts[g, nz, at, cols].astype(f32)

        @pl.loop(0, block // 64)
        def _(i):
            at = pl.ds(i * 64, 64)
            parts[g, d, at, cols] = tile[at, :].astype(bf16)

        target = jnp.where(d == z - 1, nz, d)
        device = {"fs": jnp.where(d > z, f + 2, f - 2)}
        for width, size in sizes:
            copy = links.make(
                "p",
                parts.at[g, d, :, lanes(q * cut, width)],
                parts.at[g, target, :, lanes(q * cut, width)],
                device,
                size=count,
                send_at=spot + d,
                recv_at=spot + target,
            )
            guarded(far & size, copy.start)

    def grad_sent():
        @pl.loop(0, 3 * CHUNKS)
        def _(i):
            q, g = lax.div(i, 3), lax.rem(i, 3)
            spot = i * (nz + 1)

            @pl.loop(0, nz)
            def _(d):
                for width, size in (
                    (cut, (q < tail) | wide),
                    (cut - LANE, (q == tail) & slim),
                ):
                    copy = links.make(
                        "p",
                        parts.at[g, d, :, lanes(q * cut, width)],
                        parts.at[g, d, :, lanes(q * cut, width)],
                        to_up,
                        send_at=spot + d,
                        recv_at=spot + d,
                    )
                    guarded((d != z) & size, copy.wait_send)

    out_waits = []

    def out_pieces(q, yy, extra):
        lo, hi = q * cut, min((q + 1) * cut, main)
        pieces = [("o", lo, hi - lo, yy * (main + LANE) + lo, None)]
        if q == tail:
            pieces.append(("e", main, LANE, main, extra))
        return pieces

    def spread(q, g):
        keep = parts.at[g, z, pl.ds(y * feats, feats), :]
        give = parts.at[g, z, pl.ds((1 - y) * feats, feats), :]
        for tag, start, size, col, when in out_pieces(q, y, wide):
            there = outs[g].at[:, lanes(x * half + col, size)]
            back = outs[g].at[:, lanes((1 - x) * half + col, size)]
            out_waits.append(links.here(keep.at[:, pl.ds(start, size)], there, when))
            links.start(f"h{q}{g}{tag}x", keep.at[:, pl.ds(start, size)], there, to_x, when)
            links.start(f"h{q}{g}{tag}y", give.at[:, pl.ds(start, size)], there, to_y, when)
            out_waits.append(functools.partial(links.arrive, f"h{q}{g}{tag}x", back, to_x, when))

    def spread_on(q, g):
        for tag, start, size, col, when in out_pieces(q, 1 - y, slim):
            here = outs[g].at[:, lanes(x * half + col, size)]
            back = outs[g].at[:, lanes((1 - x) * half + col, size)]
            links.arrive(f"h{q}{g}{tag}y", here, to_y, when)
            links.start(f"h{q}{g}{tag}n", here, here, to_x, when)
            out_waits.append(functools.partial(links.arrive, f"h{q}{g}{tag}n", back, to_x, when))

    def turn(i):
        return jnp.where(i < 2, 3 - 2 * i, 6 - 2 * i)

    def row_grad(core, slot, target, add):
        at = pl.ds((slot * 2 + core) * tokens, tokens)

        @pl.loop(0, 4)
        def _(n):
            wide_cols = lanes(n * (model // 4), model // 4)
            feat_rows = pl.ds(n * (model // 4), model // 4)
            value = contract_cols(acts[1, at, :], weights[1, feat_rows, :])
            value = value + contract_cols(acts[2, at, :], weights[2, feat_rows, :])
            if add:
                value = value + mate[slot, :, wide_cols].astype(f32)
            target[slot, :, wide_cols] = value.astype(bf16)

    def to_mate(slot):
        return links.make(
            "s", near.at[slot], mate.at[slot], to_c, size=4, send_at=slot, recv_at=slot
        )

    def rows_for_mate(lo, hi):
        @pl.loop(lo, hi)
        def _(i):
            slot = turn(i)
            row_grad(1 - c, slot, near, False)
            to_mate(slot).start()

    def rows_here(lo, hi):
        @pl.loop(lo, hi)
        def _(i):
            slot = turn(i)
            to_mate(slot).wait_recv()
            row_grad(c, slot, mate, True)

    def pass_on(slot, h):
        device, at = (to_y, slot // 2) if h == 0 else (to_x, slot % 2)
        links.start(
            f"t{slot}{h}", mate.at[slot, :, half_cols(h)], side.at[at, :, half_cols(h)], device
        )

    def gather_in(slot, h, last):
        there = slot + (1 if h == 0 else 2)
        device, at = (to_y, there // 2) if h == 0 else (to_x, there % 2)
        links.arrive(f"t{there}{h}", side.at[at, :, half_cols(h)], device)

        @pl.loop(0, tokens // 32)
        def _(i):
            r = pl.ds(i * 32, 32)
            value = mate[slot, r, half_cols(h)].astype(f32) + side[at, r, half_cols(h)].astype(f32)
            mate[slot, r, half_cols(h)] = value.astype(bf16)

        if not last:
            device = to_x if h == 0 else to_y
            there = distant.at[:, half_cols(h)]
            links.start(f"u{h}", mate.at[slot, :, half_cols(h)], there, device)

    def reload():
        @pl.loop(0, 4)
        def _(slot):
            to_mate(slot).wait_send()

        return [links.here(v, near.at[i]) for i, v in ((1, cotangent), (2, inputs))]

    def finish_rows(waits):
        for wait in waits:
            wait()
        for h in range(2):
            device = to_x if h == 0 else to_y
            links.arrive(f"u{h}", distant.at[:, half_cols(h)], device)

        @pl.loop(0, tokens // 16)
        def _(i):
            at = pl.ds(i * 16, 16)
            grad = mate[0, at, :].astype(f32) + distant[at, :].astype(f32)
            v = near[2, at, :].astype(f32)
            inv = lax.rsqrt(jnp.mean(v * v, axis=-1, keepdims=True) + eps)
            w = grad * pre_gain[...]
            value = near[1, at, :].astype(f32) + inv * w
            value = value - v * inv**3 * jnp.mean(w * v, axis=-1, keepdims=True)
            near[0, at, :] = value.astype(bf16)

        out_waits.append(links.here(near.at[0], rows_out))

    def grads(steps, when=None):
        @pl.loop(0, len(steps) if when is None else jnp.where(when, len(steps), 0))
        def _(i):
            k = steps[0]
            for j in range(1, len(steps)):
                k = jnp.where(i == j, steps[j], k)
            k = k + 0 * i
            grad_step(lax.div(k, 3 * nz), lax.rem(lax.div(k, nz), 3), lax.rem(k, nz))

    def settle(waits):
        for wait in waits:
            wait()

    def z_first(w, o):
        if o == 0:
            settle(own_weight[w])
        else:
            y_weight_wait(w)
        z_send(w, o, 0)

    def clear_extra():
        @pl.when(slim)
        def _():
            @pl.loop(0, total // 64)
            def _(i):
                at = pl.ds(i * 64, 64)
                for g in (1, 2):
                    acts[g, at, pl.ds(main, LANE)] = jnp.zeros((64, LANE), bf16)

            @pl.loop(0, model // 64)
            def _(i):
                at = pl.ds(i * 64, 64)
                for w in range(3):
                    weights[w, at, pl.ds(main, LANE)] = jnp.zeros((64, LANE), bf16)

    z_first(0, 0)
    act_send(2, 2)
    y_weight(0)
    settle(own_rows)
    make_rows(0)
    row_other(0, 0)
    y_weight(2)
    make_rows(1)
    clear_extra()
    row_first(0, 1)
    y_weight(1)
    row_first(0, 0)
    row_other(0, 2)
    row_first(0, 3)
    z_first(1, 0)
    row_first(0, 2)
    z_step(0, 0, 1)
    act_send(0, 2)
    z_first(2, 0)
    row_other(0, 3)
    row_relay(0, 1)
    act_send(2, 3)
    row_other(0, 1)
    z_first(0, 1)
    row_other_in(0, 0)
    act_send(2, 1)
    act_send(0, 1)
    z_step(0, 0, 2)
    z_step(0, 1, 1)
    row_last_in(0, 1)
    row_first(1, 1)
    act_send(0, 3)
    z_first(2, 1)
    row_other(1, 0)
    z_step(0, 1, 2)
    row_other_in(0, 3)
    z_first(1, 1)
    z_step(2, 0, 1)
    row_other_in(0, 1)
    row_relay(0, 0)
    row_relay(0, 3)
    row_last_in(0, 0)
    settle(own_acts)
    act_wait(2)
    make_hidden(2)
    z_step(2, 1, 1)
    z_rest(0)
    row_first(1, 0)
    row_ready(0, 1)
    row_other_in(0, 2)
    grads((25,), ends)
    row_relay(0, 2)
    row_last_in(0, 3)
    row_ready(0, 0)
    grads((24,), ends)
    act_wait(0)
    make_hidden(0)
    row_relay(1, 1)
    row_other(1, 3)
    row_relay(1, 0)
    row_ready(0, 3)
    grads((1,), ends)
    grads((24,), inner)
    act_send(1, 1)
    z_step(1, 1, 1)
    z_step(2, 0, 2)
    grads((0,), ends)
    row_last_in(0, 2)
    row_other(1, 1)
    z_step(1, 0, 1)
    row_ready(0, 2)
    grads((2,), ends)
    row_other(1, 2)
    make_cots(0)
    grads((26,), ends)
    row_other_in(1, 0)
    grads((25,), inner)
    row_last_in(1, 1)
    row_last_in(1, 0)
    grads((0, 26), inner)
    act_send(1, 3)
    make_cots(2)
    row_other_in(1, 1)
    row_ready(1, 0)
    z_step(2, 1, 2)
    grads((28,), ends)
    row_first(1, 3)
    z_step(1, 1, 2)
    row_ready(1, 1)
    row_first(1, 2)
    z_step(1, 0, 2)
    grads((32, 4, 9, 29, 8), ends)
    grads((1, 28), inner)
    row_other_in(1, 3)
    act_send(1, 2)
    row_relay(1, 2)
    grads((33, 5), ends)
    grads((2, 9, 4, 32), inner)
    grads((27,))
    spread(2, 0)
    act_wait(1)
    make_hidden(1)
    make_cots(1)
    grads((12, 16, 17), ends)
    grads((29,), inner)
    row_other_in(1, 2)
    z_rest(1)
    row_relay(1, 3)
    row_last_in(1, 2)
    z_rest(2)
    rows_for_mate(0, 2)
    grads((3,))
    spread(0, 0)
    spread_on(2, 0)
    rows_for_mate(2, 4)
    grads((5,), inner)
    spread_on(0, 0)
    rows_here(0, 2)
    pass_on(3, 0)
    pass_on(3, 1)
    pass_on(1, 0)
    row_ready(1, 2)
    grads((30,), ends)
    grads((12, 8), inner)
    row_last_in(1, 3)
    grads((20, 13, 18), ends)
    grads((6,), inner)
    rows_here(2, 4)
    pass_on(2, 1)
    grads((34,), ends)
    row_ready(1, 3)
    grads((14, 30, 17, 16, 10), inner)
    gather_in(2, 0, False)
    again = reload()
    grads((14,), ends)
    gather_in(1, 1, False)
    grads((33,), inner)
    grads((31,))
    spread(2, 1)
    gather_in(0, 1, True)
    grads((21, 6, 22), ends)
    grads((13, 34, 18, 20), inner)
    grads((35,))
    spread(2, 2)
    spread_on(2, 1)
    grads((10,), ends)
    spread_on(2, 2)
    grads((19,))
    spread(1, 1)
    grads((22,), inner)
    grads((15,))
    spread(1, 0)
    grads((21,), inner)
    spread_on(1, 1)
    grads((7,))
    spread(0, 1)
    gather_in(0, 0, True)
    finish_rows(again)
    spread_on(1, 0)
    grads((23,))
    spread(1, 2)
    spread_on(0, 1)
    grads((11,))
    spread(0, 2)
    spread_on(1, 2)
    spread_on(0, 2)
    settle(out_waits)
    grad_sent()
    links.finish()


def fused_device(nz, block_input, pre_gain, post_gain, gate_saved, up_saved, branch_saved,
                 out_cotangent, gate_weight, up_weight, down_weight):
    tokens, model = block_input.shape
    chip, width = gate_saved.shape
    feats = down_weight.shape[0]
    full = (width // 2 // LANE + 1) // 2 * LANE
    grad = jax.ShapeDtypeStruct((feats, width), bf16)
    total = jax.ShapeDtypeStruct((tokens, model), bf16)
    down_grad, gate_grad, up_grad, input_grad = pl.pallas_call(
        functools.partial(fused_kernel, nz),
        out_shape=(grad, grad, grad, total),
        in_specs=[pl.BlockSpec(memory_space=pl.ANY)] * 3
        + [pl.BlockSpec(memory_space=pltpu.VMEM)] * 2
        + [pl.BlockSpec(memory_space=pl.ANY)] * 5,
        out_specs=[pl.BlockSpec(memory_space=pl.ANY)] * 4,
        scratch_shapes=[
            pltpu.VMEM((2, 4 * chip, model), bf16),
            pltpu.VMEM((3, 4 * chip, full), bf16),
            pltpu.VMEM((3, model, full), bf16),
            pltpu.VMEM((3, nz + 1, 2 * feats, full), bf16),
            pltpu.VMEM((4, tokens, model), bf16),
            pltpu.VMEM((4, tokens, model), bf16),
            pltpu.VMEM((2, tokens, model), bf16),
            pltpu.VMEM((tokens, model), bf16),
            pltpu.VMEM((2 * feats, full // CHUNKS), f32),
            pltpu.SemaphoreType.DMA((SEMS,)),
            pltpu.SemaphoreType.DMA((SEMS,)),
            pltpu.SemaphoreType.DMA((LOCALS,)),
        ],
        compiler_params=pltpu.CompilerParams(
            collective_id=0, has_side_effects=True, vmem_limit_bytes=66_900_000
        ),
    )(
        block_input,
        branch_saved,
        out_cotangent,
        pre_gain.reshape(1, model),
        post_gain.reshape(1, model),
        gate_saved,
        up_saved,
        down_weight,
        gate_weight,
        up_weight,
    )

    return (
        input_grad,
        gate_grad.astype(f32),
        up_grad.astype(f32),
        down_grad.astype(f32),
    )


def solution(mesh):
    shape = mesh.shape

    def run(*args):
        width = args[3].shape[1] // shape["tp"]
        tiles, odd = divmod(width // 2, LANE)
        fits = shape["rep"] == 2 and shape["tp"] == 2 and shape["fs"] == 2 * LINE
        fits = fits and width % 2 == 0 and odd == 0 and tiles % 6 == 5
        if fits:
            per_device = functools.partial(fused_device, shape["fs"] // 2)
        else:
            per_device = functools.partial(plain_device, shape["rep"])
        return jax.shard_map(
            per_device,
            mesh=mesh,
            in_specs=(
                P(("rep", "fs", "tp"), None),
                P(),
                P(),
                P(("rep", "fs"), "tp"),
                P(("rep", "fs"), "tp"),
                P(("rep", "fs", "tp"), None),
                P(("rep", "fs", "tp"), None),
                P("fs", "tp"),
                P("fs", "tp"),
                P("fs", "tp"),
            ),
            out_specs=(P(("rep", "fs", "tp"), None), P("fs", "tp"), P("fs", "tp"), P("fs", "tp")),
            check_vma=False,
        )(*args)

    return run
```

```python
import functools

import jax
import jax.numpy as jnp
from jax import lax
from jax.experimental import pallas as pl
from jax.experimental.pallas import tpu as pltpu
from jax.sharding import PartitionSpec as P

eps = 1e-06
bf16, f32 = jnp.bfloat16, jnp.float32
SEMS, LOCALS = 240, 64
CHUNKS = 3
LINE = 4


def contract_rows(left, right):
    return lax.dot_general(
        left, right, (((0,), (0,)), ((), ())), preferred_element_type=jnp.float32
    )


def contract_cols(left, right):
    return lax.dot_general(
        left, right, (((1,), (1,)), ((), ())), preferred_element_type=jnp.float32
    )


def shifted(value, reps, step):
    return lax.ppermute(value, "rep", [(i, (i + step) % reps) for i in range(reps)])


def plain_device(
    reps,
    block_input,
    pre_gain,
    post_gain,
    gate_saved,
    up_saved,
    branch_saved,
    out_cotangent,
    gate_weight,
    up_weight,
    down_weight,
):
    me = lax.axis_index("rep")
    width = gate_saved.shape[1] // reps

    def columns(value, owner):
        return lax.dynamic_slice_in_dim(value, owner * width, width, axis=1)

    down_full = lax.all_gather(columns(down_weight, me), "fs", axis=0, tiled=True)

    gates = [columns(gate_saved, me)]
    ups = [columns(up_saved, me)]
    for k in range(1, reps):
        there = lax.rem(me + k, reps)
        gates.append(shifted(columns(gate_saved, there), reps, k))
        ups.append(shifted(columns(up_saved, there), reps, k))

    xfull = block_input.astype(f32)
    inv_x = lax.rsqrt(jnp.mean(xfull * xfull, axis=-1, keepdims=True) + eps)
    normed = (xfull * inv_x * pre_gain).astype(bf16)
    branch = branch_saved.astype(f32)
    inv_b = lax.rsqrt(jnp.mean(branch * branch, axis=-1, keepdims=True) + eps)
    upstream = 0.5 * out_cotangent.astype(f32) * post_gain
    branch_grad = (
        inv_b * upstream - branch * inv_b**3 * jnp.mean(upstream * branch, axis=-1, keepdims=True)
    ).astype(bf16)

    normed_own = [normed] + [shifted(normed, reps, k) for k in range(1, reps)]
    branch_own = [branch_grad] + [shifted(branch_grad, reps, k) for k in range(1, reps)]
    normed_rows = [lax.all_gather(v, "tp", axis=0, tiled=True) for v in normed_own]
    branch_rows = [lax.all_gather(v, "tp", axis=0, tiled=True) for v in branch_own]
    normed_all = jnp.concatenate(normed_rows, axis=0)
    branch_all = jnp.concatenate(branch_rows, axis=0)

    gate_f = jnp.concatenate(gates, axis=0).astype(f32)
    up_f = jnp.concatenate(ups, axis=0).astype(f32)
    sigma = jax.nn.sigmoid(gate_f)
    silu_gate = gate_f * sigma
    hidden = (silu_gate * up_f).astype(bf16)

    def spread(total):
        shard = lax.psum_scatter(total.astype(bf16), "fs", scatter_dimension=0, tiled=True)
        out = jnp.zeros((shard.shape[0], width * reps), f32)
        out = lax.dynamic_update_slice_in_dim(out, shard.astype(f32), me * width, axis=1)
        for k in range(1, reps):
            other = shifted(shard, reps, k).astype(f32)
            out = lax.dynamic_update_slice_in_dim(
                out, other, lax.rem(me - k + reps, reps) * width, axis=1
            )
        return out

    down_grad = spread(contract_rows(branch_all, hidden))

    hidden_grad = jnp.dot(branch_all, down_full, preferred_element_type=f32)
    gate_cot = (hidden_grad * up_f * sigma * (1.0 + gate_f * (1.0 - sigma))).astype(bf16)
    up_cot = (hidden_grad * silu_gate).astype(bf16)
    gate_grad = spread(contract_rows(normed_all, gate_cot))
    up_grad = spread(contract_rows(normed_all, up_cot))

    gate_full = lax.all_gather(columns(gate_weight, me), "fs", axis=0, tiled=True)
    up_full = lax.all_gather(columns(up_weight, me), "fs", axis=0, tiled=True)
    partial = (contract_cols(gate_cot, gate_full) + contract_cols(up_cot, up_full)).astype(bf16)
    rows = partial.shape[0] // reps
    normed_grad = None
    for k in range(reps):
        piece = lax.psum_scatter(
            partial[k * rows : (k + 1) * rows], "tp", scatter_dimension=0, tiled=True
        )
        if k:
            piece = shifted(piece, reps, reps - k)
        piece = piece.astype(f32)
        normed_grad = piece if normed_grad is None else normed_grad + piece

    scaled = normed_grad * pre_gain
    input_grad = (
        out_cotangent.astype(f32)
        + inv_x * scaled
        - xfull * inv_x**3 * jnp.mean(scaled * xfull, axis=-1, keepdims=True)
    )
    return (input_grad.astype(bf16), gate_grad, up_grad, down_grad)


LANE = 128
MESH = pl.DeviceIdType.MESH


class Links:
    def __init__(self, send, recv, local):
        self.send, self.recv, self.local = send, recv, local
        self.names, self.count, self.pending, self.locals = {}, 0, [], 0

    def index(self, name, size=1):
        if name not in self.names:
            self.names[name] = self.count
            self.count += size
        return self.names[name]

    def make(self, name, src, dst, device, size=1, send_at=0, recv_at=0):
        base = self.index(name, size)
        return pltpu.make_async_remote_copy(
            src_ref=src,
            dst_ref=dst,
            send_sem=self.send.at[base + send_at],
            recv_sem=self.recv.at[base + recv_at],
            device_id=device,
            device_id_type=MESH,
        )

    def start(self, name, src, dst, device, when=None, **at):
        copy = self.make(name, src, dst, device, **at)
        guarded(when, copy.start)
        self.pending.append((when, copy))

    def arrive(self, name, dst, device, when=None, **at):
        guarded(when, self.make(name, dst, dst, device, **at).wait_recv)

    def here(self, src, dst, when=None):
        copy = pltpu.make_async_copy(src, dst, self.local.at[self.locals])
        self.locals += 1
        guarded(when, copy.start)
        return lambda: guarded(when, copy.wait)

    def finish(self):
        for when, copy in self.pending:
            guarded(when, copy.wait_send)


def guarded(when, action):
    if when is None:
        action()
    else:
        pl.when(when)(action)


def fused_kernel(
    nz,
    inputs,
    branch,
    cotangent,
    pre_gain,
    post_gain,
    gate,
    up,
    down_w,
    gate_w,
    up_w,
    down_out,
    gate_out,
    up_out,
    rows_out,
    rows,
    acts,
    weights,
    parts,
    near,
    mate,
    side,
    distant,
    tile,
    send,
    recv,
    local,
):
    x, f, c = (lax.axis_index(a) for a in ("rep", "fs", "tp"))
    y, z = lax.rem(f, 2), lax.div(f, 2)
    links = Links(send, recv, local)
    to_x = {"rep": 1 - x}
    to_y = {"fs": f + 1 - 2 * y}
    to_d = {"rep": 1 - x, "fs": f + 1 - 2 * y}
    to_c = {"tp": 1 - c}
    to_up, to_dn = {"fs": f + 2}, {"fs": f - 2}
    has_up, has_dn = z < nz - 1, z > 0

    tokens, model = inputs.shape
    chip = gate.shape[0]
    feats = down_w.shape[0]
    block = 2 * feats
    half = gate.shape[1] // 2
    full = acts.shape[2]
    main = full - LANE
    cut = full // CHUNKS
    tail = CHUNKS - 1
    wide, slim = y == c, y != c
    sources = (down_w, gate_w, up_w)
    outs = (down_out, gate_out, up_out)

    def lanes(start, size):
        return pl.ds(pl.multiple_of(start, LANE), size)

    barrier = pltpu.get_barrier_semaphore()
    for device in (to_x, to_y, to_d, to_c):
        pl.semaphore_signal(barrier, inc=1, device_id=device, device_id_type=MESH)

    @pl.when(has_up)
    def _():
        pl.semaphore_signal(barrier, inc=1, device_id=to_up, device_id_type=MESH)

    @pl.when(has_dn)
    def _():
        pl.semaphore_signal(barrier, inc=1, device_id=to_dn, device_id_type=MESH)

    def own_cols(xx, yy, lo, hi):
        return lanes(xx * half + yy * (main + LANE) + lo, hi - lo)

    def extra_cols(xx):
        return lanes(xx * half + main, LANE)

    my_feats = pl.ds(f * feats, feats)
    own_weight = []
    for w in range(3):
        own_weight.append(
            (
                links.here(
                    sources[w].at[:, own_cols(x, y, 0, main)],
                    weights.at[w, my_feats, pl.ds(0, main)],
                ),
                links.here(
                    sources[w].at[:, extra_cols(x)],
                    weights.at[w, my_feats, pl.ds(main, LANE)],
                    wide,
                ),
            )
        )
    own_acts = []
    for g, saved in ((1, gate), (2, up)):
        own_acts.append(
            links.here(saved.at[:, own_cols(x, y, 0, main)], acts.at[g, pl.ds(0, chip), pl.ds(0, main)])
        )
        own_acts.append(
            links.here(
                saved.at[:, extra_cols(x)], acts.at[g, pl.ds(0, chip), pl.ds(main, LANE)], wide
            )
        )

    def slot_rows(slot, core):
        return pl.ds((slot * 2 + core) * tokens, tokens)

    own_rows = [links.here(v, near.at[i]) for i, v in enumerate((branch, cotangent, inputs))]

    def make_rows(a):
        @pl.loop(0, tokens // 16)
        def _(i):
            at = pl.ds(i * 16, 16)
            v = near[0 if a == 0 else 2, at, :].astype(f32)
            inv = lax.rsqrt(jnp.mean(v * v, axis=-1, keepdims=True) + eps)
            if a == 0:
                u = 0.5 * near[1, at, :].astype(f32) * post_gain[...]
                value = inv * u - v * inv**3 * jnp.mean(u * v, axis=-1, keepdims=True)
            else:
                value = v * inv * pre_gain[...]
            rows[a, pl.ds(c * tokens + i * 16, 16), :] = value.astype(bf16)

        for k in range(nz):
            mate_send(a, k, 0)

    pl.semaphore_wait(barrier, 4 + has_up.astype(jnp.int32) + has_dn.astype(jnp.int32))

    def order(s):
        def low(zz):
            return jnp.where(
                s < nz - 1 - zz, nz - 1 - s, jnp.where(s == nz - 1, zz, s - (nz - 1 - zz))
            )

        return jnp.where(2 * z < nz, low(z), nz - 1 - low(nz - 1 - z))

    routes = (("y", "y", "y", "y"), ("x", "y", "x", "y"))

    def half_cols(h):
        return pl.ds(h * (model // 2), model // 2)

    def row_part(a, k, slot, core):
        return rows.at[a, slot_rows(slot, core), lanes(order(k) * block, block)]

    def row_path(a, k):
        y_way, x_way = (to_y, 1), (to_x, 2)
        return (y_way, x_way) if routes[a][k] == "y" else (x_way, y_way)

    def row_first(a, k):
        (device, slot), _ = row_path(a, k)
        links.start(f"f{a}{k}", row_part(a, k, 0, c), row_part(a, k, slot, c), device)

    def row_other(a, k):
        _, (device, slot) = row_path(a, k)
        links.start(f"o{a}{k}", row_part(a, k, 0, c), row_part(a, k, slot, c), device)

    def row_relay(a, k):
        (device, slot), (onward, _) = row_path(a, k)
        links.arrive(f"f{a}{k}", row_part(a, k, slot, c), device)
        links.start(f"r{a}{k}", row_part(a, k, slot, c), row_part(a, k, 3, c), onward)
        mate_send(a, k, slot)

    def row_other_in(a, k):
        _, (device, slot) = row_path(a, k)
        links.arrive(f"o{a}{k}", row_part(a, k, slot, c), device)
        mate_send(a, k, slot)

    def row_last_in(a, k):
        _, (onward, _) = row_path(a, k)
        links.arrive(f"r{a}{k}", row_part(a, k, 3, c), onward)
        mate_send(a, k, 3)

    def mate_send(a, k, slot):
        links.start(f"m{a}{k}{slot}", row_part(a, k, slot, c), row_part(a, k, slot, c), to_c)

    def row_ready(a, k):
        for slot in range(4):
            links.arrive(f"m{a}{k}{slot}", row_part(a, k, slot, 1 - c), to_c)

    def y_weight(w):
        there = weights.at[w, my_feats, :]
        links.start(
            f"w{w}y",
            sources[w].at[:, own_cols(x, 1 - y, 0, main)],
            there.at[:, pl.ds(0, main)],
            to_y,
        )
        links.start(
            f"w{w}e", sources[w].at[:, extra_cols(x)], there.at[:, pl.ds(main, LANE)], to_y, slim
        )

    def y_weight_wait(w):
        there = weights.at[w, pl.ds((f + 1 - 2 * y) * feats, feats), :]
        links.arrive(f"w{w}y", there.at[:, pl.ds(0, main)], to_y)
        links.arrive(f"w{w}e", there.at[:, pl.ds(main, LANE)], to_y, wide)

    def weight_piece(w, origin, o, width):
        yy = y if o == 0 else 1 - y
        return weights.at[w, pl.ds((origin * 2 + yy) * feats, feats), pl.ds(0, width)]

    def z_send(w, o, hop):
        for width, size in ((full, wide), (main, slim)):
            ahead = weight_piece(w, jnp.maximum(z - hop, 0), o, width)
            when = size & has_up & (z >= hop)
            links.start(f"z{w}{o}u{hop}", ahead, ahead, to_up, when)
            behind = weight_piece(w, jnp.minimum(z + hop, nz - 1), o, width)
            when = size & has_dn & (z + hop < nz)
            links.start(f"z{w}{o}d{hop}", behind, behind, to_dn, when)

    def z_wait(w, o, hop, here):
        for width, size in ((full, wide & here), (main, slim & here)):
            ahead = weight_piece(w, jnp.maximum(z - hop, 0), o, width)
            links.arrive(f"z{w}{o}u{hop - 1}", ahead, to_up, size & (z >= hop))
            behind = weight_piece(w, jnp.minimum(z + hop, nz - 1), o, width)
            links.arrive(f"z{w}{o}d{hop - 1}", behind, to_dn, size & (z + hop < nz))

    ends = (z == 0) | (z == nz - 1)
    inner = jnp.logical_not(ends)

    def z_step(w, o, hop):
        z_wait(w, o, hop, inner)
        z_send(w, o, hop)

    def z_rest(w):
        for o in range(2):
            for hop in range(1, nz - 1):
                z_wait(w, o, hop, ends)
            z_wait(w, o, nz - 1, ends | inner)

    peers = ((2, to_x, 1 - x, y), (1, to_y, x, 1 - y), (3, to_d, 1 - x, 1 - y))

    def act_send(q, to):
        for slot, device, xx, yy in peers:
            if slot != to:
                continue
            for g, saved in ((1, gate), (2, up)):
                there = acts.at[g, pl.ds(slot * chip, chip), :]
                lo, hi = q * cut, min((q + 1) * cut, main)
                links.start(
                    f"a{q}{g}{slot}",
                    saved.at[:, own_cols(xx, yy, lo, hi)],
                    there.at[:, pl.ds(lo, hi - lo)],
                    device,
                )
                if q == tail:
                    links.start(
                        f"e{g}{slot}",
                        saved.at[:, extra_cols(xx)],
                        there.at[:, pl.ds(main, LANE)],
                        device,
                        yy == c,
                    )

    def act_wait(q):
        for slot, device, _, _ in peers:
            for g in (1, 2):
                there = acts.at[g, pl.ds(slot * chip, chip), :]
                lo, hi = q * cut, min((q + 1) * cut, main)
                links.arrive(f"a{q}{g}{slot}", there.at[:, pl.ds(lo, hi - lo)], device)
                if q == tail:
                    links.arrive(f"e{g}{slot}", there.at[:, pl.ds(main, LANE)], device, wide)

    total = acts.shape[1]

    def make_hidden(q):
        cols = pl.ds(q * cut, cut)

        @pl.loop(0, total // 64)
        def _(i):
            at = pl.ds(i * 64, 64)
            g = acts[1, at, cols].astype(f32)
            u = acts[2, at, cols].astype(f32)
            acts[0, at, cols] = (g * jax.nn.sigmoid(g) * u).astype(bf16)

    def make_cots(q):
        cols = pl.ds(q * cut, cut)

        @pl.loop(0, total // 256)
        def _(i):
            at = pl.ds(i * 256, 256)
            tile[pl.ds(0, 256), :] = jnp.dot(
                rows[0, at, :], weights[0, :, cols], preferred_element_type=f32
            )

            @pl.loop(0, 4)
            def _(j):
                sub = pl.ds(i * 256 + j * 64, 64)
                grad = tile[pl.ds(j * 64, 64), :]
                g = acts[1, sub, cols].astype(f32)
                u = acts[2, sub, cols].astype(f32)
                s = jax.nn.sigmoid(g)
                acts[1, sub, cols] = (grad * u * s * (1.0 + g * (1.0 - s))).astype(bf16)
                acts[2, sub, cols] = (grad * (g * s)).astype(bf16)

    def grad_step(q, g, s):
        d = order(s)
        cols = lanes(q * cut, cut)

        @pl.loop(0, block // 256)
        def _(m):
            tile[pl.ds(m * 256, 256), :] = contract_rows(
                rows[jnp.minimum(g, 1), :, pl.ds(pl.multiple_of(d * block + m * 256, 256), 256)],
                acts[g, :, cols],
            )

        sizes = ((cut, (q < tail) | wide), (cut - LANE, (q == tail) & slim))
        spot = (q * 3 + g) * (nz + 1)
        count = 3 * CHUNKS * (nz + 1)

        def take(slot, when):
            for width, size in sizes:
                links.arrive(
                    "p",
                    parts.at[g, slot, :, lanes(q * cut, width)],
                    to_up,
                    when & size,
                    size=count,
                    recv_at=spot + slot,
                )

        far = d != z
        fed = jnp.where(d > z, has_dn, jnp.where(d < z, has_up, has_dn))
        take(d, fed)

        @pl.loop(0, block // 64)
        def _(i):
            at = pl.ds(i * 64, 64)

            @pl.when(fed)
            def _():
                tile[at, :] += parts[g, d, at, cols].astype(f32)

        take(nz, (d == z) & has_up)

        @pl.when((d == z) & has_up)
        def _():
            @pl.loop(0, block // 64)
            def _(i):
                at = pl.ds(i * 64, 64)
                tile[at, :] += parts[g, nz, at, cols].astype(f32)

        @pl.loop(0, block // 64)
        def _(i):
            at = pl.ds(i * 64, 64)
            parts[g, d, at, cols] = tile[at, :].astype(bf16)

        target = jnp.where(d == z - 1, nz, d)
        device = {"fs": jnp.where(d > z, f + 2, f - 2)}
        for width, size in sizes:
            copy = links.make(
                "p",
                parts.at[g, d, :, lanes(q * cut, width)],
                parts.at[g, target, :, lanes(q * cut, width)],
                device,
                size=count,
                send_at=spot + d,
                recv_at=spot + target,
            )
            guarded(far & size, copy.start)

    def grad_sent():
        @pl.loop(0, 3 * CHUNKS)
        def _(i):
            q, g = lax.div(i, 3), lax.rem(i, 3)
            spot = i * (nz + 1)

            @pl.loop(0, nz)
            def _(d):
                for width, size in (
                    (cut, (q < tail) | wide),
                    (cut - LANE, (q == tail) & slim),
                ):
                    copy = links.make(
                        "p",
                        parts.at[g, d, :, lanes(q * cut, width)],
                        parts.at[g, d, :, lanes(q * cut, width)],
                        to_up,
                        send_at=spot + d,
                        recv_at=spot + d,
                    )
                    guarded((d != z) & size, copy.wait_send)

    out_waits = []

    def out_pieces(q, yy, extra):
        lo, hi = q * cut, min((q + 1) * cut, main)
        pieces = [("o", lo, hi - lo, yy * (main + LANE) + lo, None)]
        if q == tail:
            pieces.append(("e", main, LANE, main, extra))
        return pieces

    def spread(q, g):
        keep = parts.at[g, z, pl.ds(y * feats, feats), :]
        give = parts.at[g, z, pl.ds((1 - y) * feats, feats), :]
        for tag, start, size, col, when in out_pieces(q, y, wide):
            there = outs[g].at[:, lanes(x * half + col, size)]
            back = outs[g].at[:, lanes((1 - x) * half + col, size)]
            out_waits.append(links.here(keep.at[:, pl.ds(start, size)], there, when))
            links.start(f"h{q}{g}{tag}x", keep.at[:, pl.ds(start, size)], there, to_x, when)
            links.start(f"h{q}{g}{tag}y", give.at[:, pl.ds(start, size)], there, to_y, when)
            out_waits.append(functools.partial(links.arrive, f"h{q}{g}{tag}x", back, to_x, when))
            if (q, g) == (0, 2):
                links.start(f"h{q}{g}{tag}n", give.at[:, pl.ds(start, size)], there, to_d)
                far = outs[g].at[:, lanes((1 - x) * half + (1 - y) * (main + LANE) + start, size)]
                out_waits.append(functools.partial(links.arrive, f"h{q}{g}{tag}n", far, to_d))

    def spread_on(q, g):
        for tag, start, size, col, when in out_pieces(q, 1 - y, slim):
            here = outs[g].at[:, lanes(x * half + col, size)]
            back = outs[g].at[:, lanes((1 - x) * half + col, size)]
            links.arrive(f"h{q}{g}{tag}y", here, to_y, when)
            if (q, g) == (0, 2):
                continue
            links.start(f"h{q}{g}{tag}n", here, here, to_x, when)
            out_waits.append(functools.partial(links.arrive, f"h{q}{g}{tag}n", back, to_x, when))

    def turn(i):
        return jnp.where(i < 2, 3 - 2 * i, 6 - 2 * i)

    def row_grad(core, slot, target, add):
        at = pl.ds((slot * 2 + core) * tokens, tokens)

        @pl.loop(0, 4)
        def _(n):
            wide_cols = lanes(n * (model // 4), model // 4)
            feat_rows = pl.ds(n * (model // 4), model // 4)
            value = contract_cols(acts[1, at, :], weights[1, feat_rows, :])
            value = value + contract_cols(acts[2, at, :], weights[2, feat_rows, :])
            if add:
                value = value + mate[slot, :, wide_cols].astype(f32)
            target[slot, :, wide_cols] = value.astype(bf16)

    def to_mate(slot):
        return links.make(
            "s", near.at[slot], mate.at[slot], to_c, size=4, send_at=slot, recv_at=slot
        )

    def rows_for_mate(lo, hi):
        @pl.loop(lo, hi)
        def _(i):
            slot = turn(i)
            row_grad(1 - c, slot, near, False)
            to_mate(slot).start()

    def rows_here(lo, hi):
        @pl.loop(lo, hi)
        def _(i):
            slot = turn(i)
            to_mate(slot).wait_recv()
            row_grad(c, slot, mate, True)

    def pass_on(slot, h):
        device, at = (to_y, slot // 2) if h == 0 else (to_x, slot % 2)
        links.start(
            f"t{slot}{h}", mate.at[slot, :, half_cols(h)], side.at[at, :, half_cols(h)], device
        )

    def gather_in(slot, h, last):
        there = slot + (1 if h == 0 else 2)
        device, at = (to_y, there // 2) if h == 0 else (to_x, there % 2)
        links.arrive(f"t{there}{h}", side.at[at, :, half_cols(h)], device)

        @pl.loop(0, tokens // 32)
        def _(i):
            r = pl.ds(i * 32, 32)
            value = mate[slot, r, half_cols(h)].astype(f32) + side[at, r, half_cols(h)].astype(f32)
            mate[slot, r, half_cols(h)] = value.astype(bf16)

        if not last:
            device = to_x if h == 0 else to_y
            there = distant.at[:, half_cols(h)]
            links.start(f"u{h}", mate.at[slot, :, half_cols(h)], there, device)

    def reload():
        @pl.loop(0, 4)
        def _(slot):
            to_mate(slot).wait_send()

        return [links.here(v, near.at[i]) for i, v in ((1, cotangent), (2, inputs))]

    def finish_rows(waits):
        for wait in waits:
            wait()
        for h in range(2):
            device = to_x if h == 0 else to_y
            links.arrive(f"u{h}", distant.at[:, half_cols(h)], device)

        @pl.loop(0, tokens // 16)
        def _(i):
            at = pl.ds(i * 16, 16)
            grad = mate[0, at, :].astype(f32) + distant[at, :].astype(f32)
            v = near[2, at, :].astype(f32)
            inv = lax.rsqrt(jnp.mean(v * v, axis=-1, keepdims=True) + eps)
            w = grad * pre_gain[...]
            value = near[1, at, :].astype(f32) + inv * w
            value = value - v * inv**3 * jnp.mean(w * v, axis=-1, keepdims=True)
            near[0, at, :] = value.astype(bf16)

        out_waits.append(links.here(near.at[0], rows_out))

    def grads(steps, when=None):
        @pl.loop(0, len(steps) if when is None else jnp.where(when, len(steps), 0))
        def _(i):
            k = steps[0]
            for j in range(1, len(steps)):
                k = jnp.where(i == j, steps[j], k)
            k = k + 0 * i
            grad_step(lax.div(k, 3 * nz), lax.rem(lax.div(k, nz), 3), lax.rem(k, nz))

    def settle(waits):
        for wait in waits:
            wait()

    def z_first(w, o):
        if o == 0:
            settle(own_weight[w])
        else:
            y_weight_wait(w)
        z_send(w, o, 0)

    def clear_extra():
        @pl.when(slim)
        def _():
            @pl.loop(0, total // 64)
            def _(i):
                at = pl.ds(i * 64, 64)
                for g in (1, 2):
                    acts[g, at, pl.ds(main, LANE)] = jnp.zeros((64, LANE), bf16)

            @pl.loop(0, model // 64)
            def _(i):
                at = pl.ds(i * 64, 64)
                for w in range(3):
                    weights[w, at, pl.ds(main, LANE)] = jnp.zeros((64, LANE), bf16)

    z_first(0, 0)
    act_send(2, 2)
    y_weight(0)
    settle(own_rows)
    make_rows(0)
    row_other(0, 0)
    y_weight(2)
    make_rows(1)
    clear_extra()
    row_first(0, 1)
    y_weight(1)
    row_first(0, 0)
    row_other(0, 2)
    row_first(0, 3)
    z_first(1, 0)
    row_first(0, 2)
    z_step(0, 0, 1)
    act_send(0, 2)
    z_first(2, 0)
    row_other(0, 3)
    row_relay(0, 1)
    act_send(2, 3)
    row_other(0, 1)
    z_first(0, 1)
    row_other_in(0, 0)
    act_send(2, 1)
    act_send(0, 1)
    z_step(0, 0, 2)
    z_step(0, 1, 1)
    row_last_in(0, 1)
    row_first(1, 1)
    act_send(0, 3)
    z_first(2, 1)
    row_other(1, 0)
    z_step(0, 1, 2)
    row_other_in(0, 3)
    z_first(1, 1)
    z_step(2, 0, 1)
    row_other_in(0, 1)
    row_relay(0, 0)
    row_relay(0, 3)
    row_last_in(0, 0)
    settle(own_acts)
    act_wait(2)
    make_hidden(2)
    z_step(2, 1, 1)
    z_rest(0)
    row_first(1, 0)
    row_ready(0, 1)
    row_other_in(0, 2)
    grads((25,), ends)
    row_relay(0, 2)
    row_last_in(0, 3)
    row_ready(0, 0)
    grads((24,), ends)
    act_wait(0)
    make_hidden(0)
    row_relay(1, 1)
    row_other(1, 3)
    row_relay(1, 0)
    row_ready(0, 3)
    grads((1,), ends)
    grads((24,), inner)
    act_send(1, 1)
    z_step(1, 1, 1)
    z_step(2, 0, 2)
    grads((0,), ends)
    row_last_in(0, 2)
    row_other(1, 1)
    z_step(1, 0, 1)
    row_ready(0, 2)
    grads((2,), ends)
    row_other(1, 2)
    make_cots(0)
    grads((26,), ends)
    row_other_in(1, 0)
    grads((25,), inner)
    row_last_in(1, 1)
    row_last_in(1, 0)
    grads((0, 26), inner)
    act_send(1, 3)
    make_cots(2)
    row_other_in(1, 1)
    row_ready(1, 0)
    z_step(2, 1, 2)
    grads((28,), ends)
    row_first(1, 3)
    z_step(1, 1, 2)
    row_ready(1, 1)
    row_first(1, 2)
    z_step(1, 0, 2)
    grads((32, 4, 9, 29, 8), ends)
    grads((1, 28), inner)
    row_other_in(1, 3)
    act_send(1, 2)
    row_relay(1, 2)
    grads((33, 5), ends)
    grads((2, 9, 4, 32), inner)
    grads((27,))
    spread(2, 0)
    act_wait(1)
    make_hidden(1)
    make_cots(1)
    grads((12, 16, 17), ends)
    grads((29,), inner)
    row_other_in(1, 2)
    z_rest(1)
    row_relay(1, 3)
    row_last_in(1, 2)
    z_rest(2)
    rows_for_mate(0, 2)
    grads((3,))
    spread(0, 0)
    spread_on(2, 0)
    rows_for_mate(2, 4)
    grads((5,), inner)
    spread_on(0, 0)
    rows_here(0, 2)
    pass_on(3, 0)
    pass_on(3, 1)
    pass_on(1, 0)
    row_ready(1, 2)
    grads((30,), ends)
    grads((12, 8), inner)
    row_last_in(1, 3)
    grads((20, 13, 18), ends)
    grads((6,), inner)
    rows_here(2, 4)
    pass_on(2, 1)
    grads((34,), ends)
    row_ready(1, 3)
    grads((14, 30, 17, 16, 10), inner)
    gather_in(2, 0, False)
    again = reload()
    grads((14,), ends)
    gather_in(1, 1, False)
    grads((33,), inner)
    grads((31,))
    spread(2, 1)
    gather_in(0, 1, True)
    grads((21, 6, 22), ends)
    grads((13, 34, 18, 20), inner)
    grads((35,))
    spread(2, 2)
    spread_on(2, 1)
    grads((10,), ends)
    spread_on(2, 2)
    grads((19,))
    spread(1, 1)
    grads((22,), inner)
    grads((15,))
    spread(1, 0)
    grads((21,), inner)
    spread_on(1, 1)
    grads((7,))
    spread(0, 1)
    gather_in(0, 0, True)
    finish_rows(again)
    spread_on(1, 0)
    grads((23,))
    spread(1, 2)
    spread_on(0, 1)
    grads((11,))
    spread(0, 2)
    spread_on(1, 2)
    spread_on(0, 2)
    settle(out_waits)
    grad_sent()
    links.finish()


def fused_device(nz, block_input, pre_gain, post_gain, gate_saved, up_saved, branch_saved,
                 out_cotangent, gate_weight, up_weight, down_weight):
    tokens, model = block_input.shape
    chip, width = gate_saved.shape
    feats = down_weight.shape[0]
    full = (width // 2 // LANE + 1) // 2 * LANE
    grad = jax.ShapeDtypeStruct((feats, width), bf16)
    total = jax.ShapeDtypeStruct((tokens, model), bf16)
    down_grad, gate_grad, up_grad, input_grad = pl.pallas_call(
        functools.partial(fused_kernel, nz),
        out_shape=(grad, grad, grad, total),
        in_specs=[pl.BlockSpec(memory_space=pl.ANY)] * 3
        + [pl.BlockSpec(memory_space=pltpu.VMEM)] * 2
        + [pl.BlockSpec(memory_space=pl.ANY)] * 5,
        out_specs=[pl.BlockSpec(memory_space=pl.ANY)] * 4,
        scratch_shapes=[
            pltpu.VMEM((2, 4 * chip, model), bf16),
            pltpu.VMEM((3, 4 * chip, full), bf16),
            pltpu.VMEM((3, model, full), bf16),
            pltpu.VMEM((3, nz + 1, 2 * feats, full), bf16),
            pltpu.VMEM((4, tokens, model), bf16),
            pltpu.VMEM((4, tokens, model), bf16),
            pltpu.VMEM((2, tokens, model), bf16),
            pltpu.VMEM((tokens, model), bf16),
            pltpu.VMEM((2 * feats, full // CHUNKS), f32),
            pltpu.SemaphoreType.DMA((SEMS,)),
            pltpu.SemaphoreType.DMA((SEMS,)),
            pltpu.SemaphoreType.DMA((LOCALS,)),
        ],
        compiler_params=pltpu.CompilerParams(
            collective_id=0, has_side_effects=True, vmem_limit_bytes=66_900_000
        ),
    )(
        block_input,
        branch_saved,
        out_cotangent,
        pre_gain.reshape(1, model),
        post_gain.reshape(1, model),
        gate_saved,
        up_saved,
        down_weight,
        gate_weight,
        up_weight,
    )

    return (
        input_grad,
        gate_grad.astype(f32),
        up_grad.astype(f32),
        down_grad.astype(f32),
    )


def solution(mesh):
    shape = mesh.shape

    def run(*args):
        width = args[3].shape[1] // shape["tp"]
        tiles, odd = divmod(width // 2, LANE)
        fits = shape["rep"] == 2 and shape["tp"] == 2 and shape["fs"] == 2 * LINE
        fits = fits and width % 2 == 0 and odd == 0 and tiles % 6 == 5
        if fits:
            per_device = functools.partial(fused_device, shape["fs"] // 2)
        else:
            per_device = functools.partial(plain_device, shape["rep"])
        return jax.shard_map(
            per_device,
            mesh=mesh,
            in_specs=(
                P(("rep", "fs", "tp"), None),
                P(),
                P(),
                P(("rep", "fs"), "tp"),
                P(("rep", "fs"), "tp"),
                P(("rep", "fs", "tp"), None),
                P(("rep", "fs", "tp"), None),
                P("fs", "tp"),
                P("fs", "tp"),
                P("fs", "tp"),
            ),
            out_specs=(P(("rep", "fs", "tp"), None), P("fs", "tp"), P("fs", "tp"), P("fs", "tp")),
            check_vma=False,
        )(*args)

    return run
```
